32 devices in a mesh: grp: 2 (over x), ep: 16 (over z, y, core).
Axes of the slice: x: 2, y: 2, z: 4, core: 2. Of those that a mesh axis runs over, the one named last changes fastest.
Arguments:
- tokens: bfloat16 [128, 2048], P(('grp', 'ep')), parts along dimension 0, may hold values from -6 to 6
- lengths: int32 [128], P(('grp', 'ep')), parts along dimension 0, may hold values from 128 to 1024, as said below
- cache_key: bfloat16 [128, 1024, 256], P(('grp', 'ep')), parts along dimension 0, may hold values from -6 to 6
- cache_value: bfloat16 [128, 1024, 256], P(('grp', 'ep')), parts along dimension 0, may hold values from -6 to 6
- routes: int32 [128, 2], P(('grp', 'ep')), parts along dimension 0, may hold values from 0 to 3, all different within a row
- route_logits: float32 [128, 2], P(('grp', 'ep')), parts along dimension 0, may hold values from -6 to 6
- mix_gain: float32 [2048], replicated, may hold values from 0.1 to 1.9
- query_gain: float32 [64], replicated, may hold values from 0.1 to 1.9
- key_gain: float32 [64], replicated, may hold values from 0.1 to 1.9
- head_bias: float32 [16], replicated, may hold values from -9 to -3.5
- w_query: bfloat16 [2048, 1024], P('ep'), may hold values from -0.125 to 0.125
- w_key: bfloat16 [2048, 256], P('ep'), may hold values from -0.125 to 0.125
- w_value: bfloat16 [2048, 256], P('ep'), may hold values from -0.125 to 0.125
- w_out: bfloat16 [1024, 2048], P(None, 'ep'), may hold values from -0.1875 to 0.1875
- ffn_gain: float32 [2048], replicated, may hold values from 0.1 to 1.9
- w_gate: bfloat16 [2048, 28672], P(None, 'ep'), may hold values from -0.125 to 0.125
- w_up: bfloat16 [2048, 28672], P(None, 'ep'), may hold values from -0.125 to 0.125
- w_down: bfloat16 [28672, 2048], P('ep'), may hold values from -0.0625 to 0.0625
Outputs:
- output: bfloat16 [128, 2048], P(('grp', 'ep')), parts along dimension 0
- new_key: bfloat16 [128, 256], P(('grp', 'ep')), parts along dimension 0
- new_value: bfloat16 [128, 256], P(('grp', 'ep')), parts along dimension 0
The draws below stay inside these ranges and needn't reach their ends.
There are 2 independent parts, one for each index of `grp`. The reference program is written for one: setup_inputs(seed, part) draws one part's arguments, and reference() takes and returns one part's arrays. A program takes and returns all parts, laid end to end along the dimension named above; an argument that names none is the same for every part. Nothing has to cross between parts.
Inputs may be any that keep to these rules, and one draw needn't show every extreme that they name: `lengths`: some sequence has all 1024 positions live.
All inputs are finite; a program needn't handle non-finite values.
Results may differ from the reference program's by a relative error of at most 0.0085.
Values may be sent and summed in bfloat16 or wider, within the bound.
A program may use at most 128 MiB of HBM per device.

```python
import jax
import jax.numpy as jnp
from jax import lax

D = 2048
HEADS = 16
KV_HEADS = 4
HEAD_DIM = 64
FF = 7168
EXPERTS = 4
TOP = 2
CACHE_LEN = 1024
BATCH = 64


def draw_lengths(key, part):
    spread = jax.random.randint(key, (BATCH,), CACHE_LEN // 8, CACHE_LEN + 1)
    chosen = jax.random.randint(jax.random.fold_in(key, 7), (), 0, BATCH)
    return jnp.where(jnp.arange(BATCH) == chosen, CACHE_LEN, spread).astype(jnp.int32)


def draw_head_bias(key, part):
    picker = jax.random.uniform(jax.random.fold_in(key, 1), (HEADS,), jnp.float32)
    quick = jax.random.uniform(jax.random.fold_in(key, 2), (HEADS,), jnp.float32, -4.5, -3.5)
    steady = jax.random.uniform(jax.random.fold_in(key, 3), (HEADS,), jnp.float32, -9.0, -7.5)
    portion = 0.5
    return jnp.where(picker < portion, quick, steady).astype(jnp.float32)


def steps_of(rng, dims, split, low, top_value):
    level, own = 1.0, jax.random.fold_in(rng, 6)
    for dim, parts in split:
        steps = jnp.exp(jax.random.uniform(jax.random.fold_in(own, dim), (parts,), jnp.float32, low / len(split), top_value / len(split)))
        level = level * jnp.repeat(steps, dims[dim] // parts).reshape([-1 if axis == dim else 1 for axis in range(len(dims))])
    return level


def distinct(key, rows, number_of, top, lift):
    ranking = jax.random.permutation(jax.random.fold_in(key, 1), number_of)
    favour = ranking
    for power in range(3):
        favour = favour * favour // number_of
    favour = favour * lift // number_of
    tickets = jax.random.randint(jax.random.fold_in(key, 2), (rows, number_of), 0, 4096) + favour
    fixed_rows = jax.random.permutation(jax.random.fold_in(key, 3), rows)[jnp.arange(number_of) % rows]
    tickets = jnp.where(jnp.arange(rows)[:, None] == fixed_rows[None, :], 1 << 14, tickets)
    priority = tickets * number_of + jnp.arange(number_of)
    return lax.top_k(priority.astype(jnp.int32), top)[1].astype(jnp.int32)


def normal_values(rng, dims, scale, bound, cuts=(), held_as=jnp.bfloat16):
    entries = scale * jax.random.normal(rng, dims, jnp.float32)
    if cuts:
        entries = entries * steps_of(rng, dims, cuts, -0.22, 0.18)
    return jnp.clip(entries, -bound, bound).astype(held_as)


def setup_inputs(seed: int = 0, part: int = 0) -> dict:
    arg_keys = jax.random.split(jax.random.key(seed), 19)
    part_keys = jax.random.split(jax.random.fold_in(arg_keys[18], part), 19)
    return {
        "tokens": normal_values(part_keys[0], (BATCH, D), 1.0, 6.0, ((0, 16),)),
        "lengths": draw_lengths(jax.random.fold_in(jax.random.fold_in(arg_keys[18], part), 71), part),
        "cache_key": normal_values(part_keys[2], (BATCH, CACHE_LEN, KV_HEADS * HEAD_DIM), 1.0, 6.0, ((0, 16),)),
        "cache_value": normal_values(part_keys[3], (BATCH, CACHE_LEN, KV_HEADS * HEAD_DIM), 1.0, 6.0, ((0, 16),)),
        "routes": distinct(part_keys[4], BATCH, EXPERTS, TOP, 4096),
        "route_logits": normal_values(part_keys[5], (BATCH, TOP), 1.5, 6.0, ((0, 16),), jnp.float32),
        "mix_gain": jnp.clip(1.0 + 0.18 * jax.random.normal(arg_keys[6], (D,), jnp.float32), 0.1, 1.9),
        "query_gain": jnp.clip(1.0 + 0.18 * jax.random.normal(arg_keys[7], (HEAD_DIM,), jnp.float32), 0.1, 1.9),
        "key_gain": jnp.clip(1.0 + 0.18 * jax.random.normal(arg_keys[8], (HEAD_DIM,), jnp.float32), 0.1, 1.9),
        "head_bias": draw_head_bias(jax.random.fold_in(arg_keys[18], 71), part),
        "w_query": normal_values(arg_keys[10], (D, HEADS * HEAD_DIM), D ** -0.5, 0.125, ((0, 16),)),
        "w_key": normal_values(arg_keys[11], (D, KV_HEADS * HEAD_DIM), D ** -0.5, 0.125, ((0, 16),)),
        "w_value": normal_values(arg_keys[12], (D, KV_HEADS * HEAD_DIM), D ** -0.5, 0.125, ((0, 16),)),
        "w_out": normal_values(arg_keys[13], (HEADS * HEAD_DIM, D), (HEADS * HEAD_DIM) ** -0.5, 0.1875, ((1, 16),)),
        "ffn_gain": jnp.clip(1.0 + 0.18 * jax.random.normal(arg_keys[14], (D,), jnp.float32), 0.1, 1.9),
        "w_gate": normal_values(arg_keys[15], (D, EXPERTS * FF), D ** -0.5, 0.125, ((1, 16),)),
        "w_up": normal_values(arg_keys[16], (D, EXPERTS * FF), D ** -0.5, 0.125, ((1, 16),)),
        "w_down": normal_values(arg_keys[17], (EXPERTS * FF, D), FF ** -0.5, 0.0625, ((0, 16),)),
    }


EPSILON = 1e-06

def rms_scaled(values, gain):
    return values * lax.rsqrt(lax.optimization_barrier(jnp.mean(values * values, axis=-1, keepdims=True)) + EPSILON) * gain

def route_weights(routes, route_logits):
    experts_iota = jnp.arange(EXPERTS, dtype=jnp.int32)[None, :]
    first_share = jax.nn.sigmoid(route_logits[:, 0:1] - route_logits[:, 1:2])
    second_share = jax.nn.sigmoid(route_logits[:, 1:2] - route_logits[:, 0:1])
    return jnp.where(routes[:, 0:1] == experts_iota, first_share, 0.0) + jnp.where(routes[:, 1:2] == experts_iota, second_share, 0.0)

def reference(tokens, lengths, cache_key, cache_value, routes, route_logits, mix_gain, query_gain, key_gain, head_bias, w_query, w_key, w_value, w_out, ffn_gain, w_gate, w_up, w_down):
    as_float = tokens.astype(jnp.float32)
    normed = rms_scaled(as_float, mix_gain).astype(jnp.bfloat16)
    queries = jnp.dot(normed, w_query, preferred_element_type=jnp.float32)
    fresh_key = jnp.dot(normed, w_key, preferred_element_type=jnp.float32)
    fresh_value = jnp.dot(normed, w_value, preferred_element_type=jnp.float32)
    batch_rows = tokens.shape[0]
    group_size = HEADS // KV_HEADS
    normed_query = rms_scaled(queries.reshape(batch_rows, HEADS, HEAD_DIM), query_gain).astype(jnp.bfloat16)
    normed_query = normed_query.reshape(batch_rows, KV_HEADS, group_size, HEAD_DIM)
    new_key = rms_scaled(fresh_key.reshape(batch_rows, KV_HEADS, HEAD_DIM), key_gain)
    new_key = new_key.reshape(batch_rows, KV_HEADS * HEAD_DIM).astype(jnp.bfloat16)
    new_value = fresh_value.astype(jnp.bfloat16)
    key_heads = cache_key.reshape(batch_rows, CACHE_LEN, KV_HEADS, HEAD_DIM).astype(jnp.float32)
    value_heads = cache_value.reshape(batch_rows, CACHE_LEN, KV_HEADS, HEAD_DIM).astype(jnp.float32)
    scores = jnp.einsum('bkgd,blkd->bkgl', normed_query.astype(jnp.float32), key_heads) * HEAD_DIM ** (-0.5)
    scores = scores + head_bias.reshape(KV_HEADS, group_size)[None, :, :, None]
    live_mask = jnp.arange(CACHE_LEN, dtype=jnp.int32)[None, None, None, :] < lengths.astype(jnp.int32)[:, None, None, None]
    remain = jnp.where(live_mask, jax.nn.log_sigmoid(-scores), 0.0)
    after_sum = lax.cumsum(remain, axis=3, reverse=True) - remain
    weights = jnp.where(live_mask, jnp.exp(jax.nn.log_sigmoid(scores) + after_sum), 0.0).astype(jnp.bfloat16)
    attended = jnp.einsum('bkgl,blkd->bkgd', weights.astype(jnp.float32), value_heads)
    attended = attended.reshape(batch_rows, HEADS * HEAD_DIM).astype(jnp.bfloat16)
    mixed = as_float + jnp.dot(attended, w_out, preferred_element_type=jnp.float32)
    expert_in = rms_scaled(mixed, ffn_gain).astype(jnp.bfloat16)
    gate_table = route_weights(routes, route_logits)
    expert_sum = jnp.zeros_like(mixed)
    for expert in range(EXPERTS):
        gate_value = jnp.dot(expert_in, w_gate[:, expert * FF:(expert + 1) * FF], preferred_element_type=jnp.float32)
        up_value = jnp.dot(expert_in, w_up[:, expert * FF:(expert + 1) * FF], preferred_element_type=jnp.float32)
        hidden = (jax.nn.silu(gate_value) * up_value * gate_table[:, expert:expert + 1]).astype(jnp.bfloat16)
        expert_sum = expert_sum + jnp.dot(hidden, w_down[expert * FF:(expert + 1) * FF], preferred_element_type=jnp.float32)
    return ((mixed + expert_sum).astype(jnp.bfloat16), new_key, new_value)
```

```python
import functools

import jax
import jax.numpy as jnp
from jax import lax
from jax.experimental import pallas as pl
from jax.experimental.pallas import tpu as pltpu
from jax.sharding import PartitionSpec as P

HEADS = 16
KV_HEADS = 4
HEAD_DIM = 64
FF = 7168
EXPERTS = 4


EPSILON = 1e-06


def rms_scaled(values, gain):
    return values * lax.rsqrt(jnp.mean(values * values, axis=-1, keepdims=True) + EPSILON) * gain


def route_weights(routes, route_logits):
    experts_iota = jnp.arange(EXPERTS, dtype=jnp.int32)[None, :]
    first_share = jax.nn.sigmoid(route_logits[:, 0:1] - route_logits[:, 1:2])
    second_share = jax.nn.sigmoid(route_logits[:, 1:2] - route_logits[:, 0:1])
    return jnp.where(routes[:, 0:1] == experts_iota, first_share, 0.0) + jnp.where(
        routes[:, 1:2] == experts_iota, second_share, 0.0
    )


def stick_attend(queries, lengths, cache_key, cache_value, query_gain, head_bias):
    batch_rows = queries.shape[0]
    cache_len = cache_key.shape[1]
    group_size = HEADS // KV_HEADS
    normed_query = rms_scaled(queries.reshape(batch_rows, HEADS, HEAD_DIM), query_gain).astype(
        jnp.bfloat16
    )
    normed_query = normed_query.reshape(batch_rows, KV_HEADS, group_size, HEAD_DIM)
    key_heads = cache_key.reshape(batch_rows, cache_len, KV_HEADS, HEAD_DIM)
    value_heads = cache_value.reshape(batch_rows, cache_len, KV_HEADS, HEAD_DIM)
    scores = jnp.einsum(
        "bkgd,blkd->bkgl", normed_query, key_heads, preferred_element_type=jnp.float32
    ) * HEAD_DIM ** (-0.5)
    scores = scores + head_bias.reshape(KV_HEADS, group_size)[None, :, :, None]
    live_mask = (
        jnp.arange(cache_len, dtype=jnp.int32)[None, None, None, :] < lengths[:, None, None, None]
    )
    remain = jnp.where(live_mask, jax.nn.log_sigmoid(-scores), 0.0)
    after_sum = lax.cumsum(remain, axis=3, reverse=True) - remain
    weights = jnp.where(live_mask, jnp.exp(jax.nn.log_sigmoid(scores) + after_sum), 0.0).astype(
        jnp.bfloat16
    )
    attended = jnp.einsum(
        "bkgl,blkd->bkgd", weights, value_heads, preferred_element_type=jnp.float32
    )
    return attended.reshape(batch_rows, HEADS * HEAD_DIM).astype(jnp.bfloat16)


def plain(
    tokens,
    lengths,
    cache_key,
    cache_value,
    routes,
    route_logits,
    mix_gain,
    query_gain,
    key_gain,
    head_bias,
    w_query,
    w_key,
    w_value,
    w_out,
    ffn_gain,
    w_gate,
    w_up,
    w_down,
):
    token_rows = tokens.shape[0]
    key_width = w_key.shape[1]
    as_float = tokens.astype(jnp.float32)
    normed = rms_scaled(as_float, mix_gain).astype(jnp.bfloat16)
    pieces = (
        lax.all_gather(w_query, "ep", axis=0, tiled=True),
        lax.all_gather(w_key, "ep", axis=0, tiled=True),
        lax.all_gather(w_value, "ep", axis=0, tiled=True),
    )
    queries, fresh_key, fresh_value = tuple(
        (jnp.dot(normed, weight, preferred_element_type=jnp.float32) for weight in pieces)
    )
    new_key = rms_scaled(fresh_key.reshape(token_rows, KV_HEADS, HEAD_DIM), key_gain)
    new_key = new_key.reshape(token_rows, key_width).astype(jnp.bfloat16)
    new_value = fresh_value.astype(jnp.bfloat16)
    attended = stick_attend(queries, lengths, cache_key, cache_value, query_gain, head_bias)
    mixed = as_float + jnp.dot(
        attended,
        lax.all_gather(w_out, "ep", axis=1, tiled=True),
        preferred_element_type=jnp.float32,
    )
    expert_in = rms_scaled(mixed, ffn_gain).astype(jnp.bfloat16)
    every_gate = lax.all_gather(route_weights(routes, route_logits), "ep", axis=0, tiled=True)
    ff_share = w_gate.shape[1]
    my_expert = lax.axis_index("ep") // (FF // ff_share)
    my_gate = lax.dynamic_slice_in_dim(every_gate, my_expert, 1, 1)
    input_rows = lax.all_gather(expert_in, "ep", axis=0, tiled=True)
    gate_value = jnp.dot(input_rows, w_gate, preferred_element_type=jnp.float32)
    up_value = jnp.dot(input_rows, w_up, preferred_element_type=jnp.float32)
    hidden = (jax.nn.silu(gate_value) * up_value * my_gate).astype(jnp.bfloat16)
    expert_sum = lax.psum_scatter(
        jnp.dot(hidden, w_down, preferred_element_type=jnp.float32),
        "ep",
        scatter_dimension=0,
        tiled=True,
    )
    return ((mixed + expert_sum).astype(jnp.bfloat16), new_key, new_value)


WEIGHT_PARTS = 4
DOWN_PARTS = 4
COLUMNS = 256


def dot(left, right):
    return jnp.dot(left, right, preferred_element_type=jnp.float32)


def iota(shape, dim):
    return lax.broadcasted_iota(jnp.int32, shape, dim)


def fused(
    n,
    tokens_ref,
    lengths_ref,
    ck_hbm,
    cv_hbm,
    routes_ref,
    logits_ref,
    mix_gain_ref,
    query_gain_ref,
    key_gain_ref,
    head_bias_ref,
    wq_hbm,
    wk_hbm,
    wv_hbm,
    wo_hbm,
    ffn_gain_ref,
    wg_hbm,
    wu_hbm,
    wd_hbm,
    out_ref,
    new_key_ref,
    new_value_ref,
    wq,
    wk,
    wv,
    wo,
    ck,
    cv,
    wg,
    wu,
    wd,
    s1,
    r1,
    s2,
    r2,
    r3,
    r4,
    s5,
    r5,
    token_cols,
    aux_rows,
    attended_rows,
    expert_in,
    hidden,
    small_sem,
    key_sem,
    value_sem,
    weight_sem,
    send_sem,
    recv_sem,
):
    me = lax.axis_index("ep")
    rows, width = tokens_ref.shape
    all_rows = rows * n
    share = width // n
    q_width = wq.shape[1]
    k_width = wk.shape[1]
    cache_len = ck.shape[1]
    group_size = HEADS // KV_HEADS
    ff_share = wg.shape[1]
    my_expert = me // (FF // ff_share)

    barrier = pltpu.get_barrier_semaphore()
    for d in range(1, n):
        pl.semaphore_signal(
            barrier,
            inc=1,
            device_id={"ep": lax.rem(me + d, n)},
            device_id_type=pl.DeviceIdType.MESH,
        )

    small = [
        pltpu.make_async_copy(a, b, small_sem.at[i])
        for i, (a, b) in enumerate(((wq_hbm, wq), (wk_hbm, wk), (wv_hbm, wv), (wo_hbm, wo)))
    ]
    for c in small[:3]:
        c.start()
    keys = [pltpu.make_async_copy(ck_hbm.at[b], ck.at[b], key_sem.at[b]) for b in range(rows)]
    values = [pltpu.make_async_copy(cv_hbm.at[b], cv.at[b], value_sem.at[b]) for b in range(rows)]
    for c in keys + values + small[3:]:
        c.start()
    weights = []
    for which, (a, b) in enumerate(((wg_hbm, wg), (wu_hbm, wu), (wd_hbm, wd))):
        step = b.shape[0] // WEIGHT_PARTS
        for part in range(WEIGHT_PARTS):
            piece = pl.ds(part * step, step)
            weights.append(
                pltpu.make_async_copy(
                    a.at[piece], b.at[piece], weight_sem.at[which, part]
                )
            )
    for c in weights:
        c.start()

    sent = []

    def send(stage, d, source, target):
        copy = pltpu.make_async_remote_copy(
            src_ref=source,
            dst_ref=target,
            send_sem=send_sem.at[stage, d],
            recv_sem=recv_sem.at[stage, me],
            device_id={"ep": lax.rem(me + d, n)},
            device_id_type=pl.DeviceIdType.MESH,
        )
        copy.start()
        sent.append(copy)

    def arrive(stage, d, target_of):
        source = lax.rem(me + d, n)
        pltpu.make_async_remote_copy(
            src_ref=target_of(source),
            dst_ref=target_of(source),
            send_sem=send_sem.at[stage, d],
            recv_sem=recv_sem.at[stage, source],
            device_id={"ep": source},
            device_id_type=pl.DeviceIdType.MESH,
        ).wait_recv()

    as_float = tokens_ref[...].astype(jnp.float32)
    scale = lax.rsqrt(jnp.mean(as_float * as_float, axis=1, keepdims=True) + EPSILON)
    lane = iota((rows, 128), 1)
    logit_gap = logits_ref[:, 0:1] - logits_ref[:, 1:2]
    first_share = 1.0 / (1.0 + jnp.exp(-logit_gap))
    second_share = 1.0 / (1.0 + jnp.exp(logit_gap))
    expert_lane = lane % EXPERTS
    gates = jnp.where(routes_ref[:, 0:1] == expert_lane, first_share, 0.0) + jnp.where(
        routes_ref[:, 1:2] == expert_lane, second_share, 0.0
    )
    aux = jnp.where(lane < 3 * EXPERTS, gates, scale)
    high = aux.astype(jnp.bfloat16).astype(jnp.float32)
    middle = (aux - high).astype(jnp.bfloat16).astype(jnp.float32)
    low = aux - high - middle
    term = jnp.where(lane < 3 * EXPERTS, lane // EXPERTS, lane - 3 * EXPERTS)
    aux = jnp.where(term == 0, high, jnp.where(term == 1, middle, low))
    for peer in range(n):
        block = jnp.concatenate(
            [as_float[:, peer * share : (peer + 1) * share], aux], axis=0
        ).astype(jnp.bfloat16)
        s1[peer] = block
    pl.semaphore_wait(barrier, n - 1)
    for d in range(1, n):
        send(0, d, s1.at[lax.rem(me + d, n)], r1.at[me])
    r1[me] = s1[me]
    for c in small[:3]:
        c.wait()
    for d in range(1, n):
        arrive(0, d, lambda source: r1.at[source])
    for peer in range(n):
        block = r1[peer].astype(jnp.float32)
        token_cols[peer * rows : (peer + 1) * rows, :] = block[:rows]
        aux_rows[peer * rows : (peer + 1) * rows, :] = block[rows:]
    aux = aux_rows[...]
    lane = iota(aux.shape, 1)
    row_scale = jnp.sum(
        jnp.where((lane >= 3 * EXPERTS) & (lane < 3 * EXPERTS + 3), aux, 0.0), axis=1, keepdims=True
    )
    my_gate = jnp.sum(
        jnp.where((lane < 3 * EXPERTS) & (lane % EXPERTS == my_expert), aux, 0.0),
        axis=1,
        keepdims=True,
    )
    my_gain = mix_gain_ref[:, pl.ds(pl.multiple_of(me * share, share), share)]
    normed = (token_cols[...] * row_scale * my_gain).astype(jnp.bfloat16)

    for weight, start in ((wq, 0), (wk, q_width), (wv, q_width + k_width)):
        partial = dot(normed, weight[...])
        for peer in range(n):
            s2[peer, :, start : start + weight.shape[1]] = partial[
                peer * rows : (peer + 1) * rows
            ].astype(jnp.bfloat16)
    for d in range(1, n):
        send(1, d, s2.at[lax.rem(me + d, n)], r2.at[me])
    r2[me] = s2[me]

    head_of_lane = iota((HEADS, q_width), 1) // HEAD_DIM
    own_lane = head_of_lane == iota((HEADS, q_width), 0)
    source_lane = iota((q_width, k_width), 0)
    target_lane = iota((q_width, k_width), 1)
    fold = jnp.where(
        (source_lane // (HEAD_DIM * group_size) == target_lane // HEAD_DIM)
        & (source_lane % HEAD_DIM == target_lane % HEAD_DIM),
        1.0,
        0.0,
    ).astype(jnp.bfloat16)
    later = jnp.where(
        iota((COLUMNS, COLUMNS), 0) > iota((COLUMNS, COLUMNS), 1), 1.0, 0.0
    ).astype(jnp.bfloat16)
    query_gain = jnp.concatenate([query_gain_ref[...]] * HEADS, axis=1)
    key_gain = jnp.concatenate([key_gain_ref[...]] * KV_HEADS, axis=1)

    for d in range(1, n):
        arrive(1, d, lambda source: r2.at[source])
    total = r2[0].astype(jnp.float32)
    for peer in range(1, n):
        total = total + r2[peer].astype(jnp.float32)
    queries = total[:, :q_width]
    fresh_key = total[:, q_width : q_width + k_width]
    new_value_ref[...] = total[:, q_width + k_width :].astype(jnp.bfloat16)
    squares = fresh_key * fresh_key
    key_lane = iota(squares.shape, 1) // HEAD_DIM
    key_scale = jnp.zeros_like(squares)
    for g in range(KV_HEADS):
        mean = jnp.sum(jnp.where(key_lane == g, squares, 0.0), axis=1, keepdims=True) / HEAD_DIM
        key_scale = jnp.where(key_lane == g, lax.rsqrt(mean + EPSILON), key_scale)
    new_key_ref[...] = (fresh_key * key_scale * key_gain).astype(jnp.bfloat16)

    spread = []
    for b in range(rows):
        wide = jnp.where(own_lane, jnp.broadcast_to(queries[b : b + 1], own_lane.shape), 0.0)
        mean = jnp.sum(wide * wide, axis=1, keepdims=True) / HEAD_DIM
        spread.append((wide * lax.rsqrt(mean + EPSILON) * query_gain).astype(jnp.bfloat16))
    folded = dot(jnp.concatenate(spread, axis=0), fold).astype(jnp.bfloat16)
    blocks = cache_len // COLUMNS
    position = iota((HEADS, cache_len), 1)
    own_group = iota((HEADS, k_width), 1) // HEAD_DIM == iota((HEADS, k_width), 0) // group_size
    heads = []
    for b in range(rows):
        keys[b].wait()
        scores = lax.dot_general(
            folded[b * HEADS : (b + 1) * HEADS],
            ck[b],
            (((1,), (1,)), ((), ())),
            preferred_element_type=jnp.float32,
        ) * HEAD_DIM ** (-0.5)
        scores = scores + head_bias_ref[...]
        live = position < lengths_ref[b]
        tail_log = jnp.log1p(jnp.exp(-jnp.abs(scores)))
        remain = jnp.where(live, jnp.minimum(-scores, 0.0) - tail_log, 0.0)
        stacked = jnp.concatenate(
            [remain[:, i * COLUMNS : (i + 1) * COLUMNS] for i in range(blocks)], axis=0
        )
        high = stacked.astype(jnp.bfloat16)
        rest = stacked - high.astype(jnp.float32)
        middle = rest.astype(jnp.bfloat16)
        low = (rest - middle.astype(jnp.float32)).astype(jnp.bfloat16)
        sums = dot(jnp.concatenate([high, middle, low], axis=0), later)
        count = blocks * HEADS
        sums = sums[:count] + sums[count : 2 * count] + sums[2 * count :]
        totals = jnp.sum(stacked, axis=1, keepdims=True)
        after = [None] * blocks
        carry = jnp.zeros((HEADS, 1), jnp.float32)
        for i in reversed(range(blocks)):
            after[i] = sums[i * HEADS : (i + 1) * HEADS] + carry
            carry = carry + totals[i * HEADS : (i + 1) * HEADS]
        after_sum = jnp.concatenate(after, axis=1)
        chance = jnp.exp(jnp.minimum(scores, 0.0) - tail_log + after_sum)
        weight = jnp.where(live, chance, 0.0).astype(jnp.bfloat16)
        values[b].wait()
        mixed_heads = dot(weight, cv[b])
        heads.append(jnp.where(own_group, mixed_heads, 0.0).astype(jnp.bfloat16))
    unfolded = lax.dot_general(
        jnp.concatenate(heads, axis=0),
        fold,
        (((1,), (1,)), ((), ())),
        preferred_element_type=jnp.float32,
    )
    attended = [
        jnp.sum(
            jnp.where(own_lane, unfolded[b * HEADS : (b + 1) * HEADS], 0.0), axis=0, keepdims=True
        )
        for b in range(rows)
    ]
    r3[me] = jnp.concatenate(attended, axis=0).astype(jnp.bfloat16)

    for d in range(1, n):
        send(2, d, r3.at[me], r3.at[me])
    small[3].wait()
    for d in range(1, n):
        arrive(2, d, lambda source: r3.at[source])
    for peer in range(n):
        attended_rows[peer * rows : (peer + 1) * rows, :] = r3[peer].astype(jnp.float32)
    mixed = token_cols[...] + dot(attended_rows[...].astype(jnp.bfloat16), wo[...])
    r4[me] = mixed.astype(jnp.bfloat16)

    for d in range(1, n):
        send(3, d, r4.at[me], r4.at[me])
    for d in range(1, n):
        arrive(3, d, lambda source: r4.at[source])
    squares = jnp.zeros((all_rows, share), jnp.float32)
    for peer in range(n):
        block = r4[peer].astype(jnp.float32)
        squares = squares + block * block
    scale = lax.rsqrt(jnp.sum(squares, axis=1, keepdims=True) / width + EPSILON)
    pick = jnp.where(
        iota((8, all_rows), 1) == iota((8, all_rows), 0) + me * rows, 1.0, 0.0
    ).astype(jnp.bfloat16)
    own_mixed = []
    for peer in range(n):
        columns = slice(peer * share, (peer + 1) * share)
        block = r4[peer]
        own_mixed.append(dot(pick, block)[:rows])
        expert_in[:, columns] = (
            block.astype(jnp.float32) * scale * ffn_gain_ref[:, columns]
        ).astype(jnp.bfloat16)
    own_mixed = jnp.concatenate(own_mixed, axis=1)

    for c in weights[: 2 * WEIGHT_PARTS]:
        c.wait()

    def hidden_step(i, carry):
        columns = pl.ds(pl.multiple_of(i * COLUMNS, COLUMNS), COLUMNS)
        gate_value = dot(expert_in[...], wg[:, columns])
        up_value = dot(expert_in[...], wu[:, columns])
        silu = gate_value / (1.0 + jnp.exp(-gate_value))
        hidden[:, columns] = (silu * up_value * my_gate).astype(jnp.bfloat16)
        return carry

    lax.fori_loop(0, ff_share // COLUMNS, hidden_step, 0)

    for c in weights[2 * WEIGHT_PARTS :]:
        c.wait()

    step = width // DOWN_PARTS
    for part in range(DOWN_PARTS):
        partial = dot(hidden[...], wd[:, part * step : (part + 1) * step])
        for peer in range(n):
            s5[part, peer] = partial[peer * rows : (peer + 1) * rows].astype(jnp.bfloat16)
        for d in range(1, n):
            send(4 + part, d, s5.at[part, lax.rem(me + d, n)], r5.at[part, me])
        r5[part, me] = s5[part, me]
    for part in range(DOWN_PARTS):
        for d in range(1, n):
            arrive(4 + part, d, lambda source: r5.at[part, source])
        total = own_mixed[:, part * step : (part + 1) * step]
        for peer in range(n):
            total = total + r5[part, peer].astype(jnp.float32)
        out_ref[:, part * step : (part + 1) * step] = total.astype(jnp.bfloat16)
    for copy in sent:
        copy.wait_send()


def local(
    n,
    tokens,
    lengths,
    cache_key,
    cache_value,
    routes,
    route_logits,
    mix_gain,
    query_gain,
    key_gain,
    head_bias,
    w_query,
    w_key,
    w_value,
    w_out,
    ffn_gain,
    w_gate,
    w_up,
    w_down,
):
    rows, width = tokens.shape
    all_rows = rows * n
    share = width // n
    q_width, k_width = w_query.shape[1], w_key.shape[1]
    wide = q_width + k_width + w_value.shape[1]
    stages = 4 + DOWN_PARTS
    vmem, anywhere = pl.BlockSpec(memory_space=pltpu.VMEM), pl.BlockSpec(memory_space=pl.ANY)
    smem = pl.BlockSpec(memory_space=pltpu.SMEM)
    bf16, f32 = jnp.bfloat16, jnp.float32

    def like(array):
        return pltpu.VMEM(array.shape, array.dtype)

    flops = 2 * all_rows * 3 * w_gate.shape[0] * w_gate.shape[1]
    return pl.pallas_call(
        functools.partial(fused, n),
        out_shape=(
            jax.ShapeDtypeStruct((rows, width), bf16),
            jax.ShapeDtypeStruct((rows, k_width), bf16),
            jax.ShapeDtypeStruct((rows, w_value.shape[1]), bf16),
        ),
        in_specs=[
            vmem,
            smem,
            anywhere,
            anywhere,
            vmem,
            vmem,
            vmem,
            vmem,
            vmem,
            vmem,
            anywhere,
            anywhere,
            anywhere,
            anywhere,
            vmem,
            anywhere,
            anywhere,
            anywhere,
        ],
        out_specs=(vmem, vmem, vmem),
        scratch_shapes=[
            like(w_query),
            like(w_key),
            like(w_value),
            like(w_out),
            like(cache_key),
            like(cache_value),
            like(w_gate),
            like(w_up),
            like(w_down),
            pltpu.VMEM((n, 2 * rows, share), bf16),
            pltpu.VMEM((n, 2 * rows, share), bf16),
            pltpu.VMEM((n, rows, wide), bf16),
            pltpu.VMEM((n, rows, wide), bf16),
            pltpu.VMEM((n, rows, q_width), bf16),
            pltpu.VMEM((n, all_rows, share), bf16),
            pltpu.VMEM((DOWN_PARTS, n, rows, width // DOWN_PARTS), bf16),
            pltpu.VMEM((DOWN_PARTS, n, rows, width // DOWN_PARTS), bf16),
            pltpu.VMEM((all_rows, share), f32),
            pltpu.VMEM((all_rows, share), f32),
            pltpu.VMEM((all_rows, q_width), f32),
            pltpu.VMEM((all_rows, width), bf16),
            pltpu.VMEM((all_rows, w_gate.shape[1]), bf16),
            pltpu.SemaphoreType.DMA((4,)),
            pltpu.SemaphoreType.DMA((rows,)),
            pltpu.SemaphoreType.DMA((rows,)),
            pltpu.SemaphoreType.DMA((3, WEIGHT_PARTS)),
            pltpu.SemaphoreType.DMA((stages, n)),
            pltpu.SemaphoreType.DMA((stages, n)),
        ],
        compiler_params=pltpu.CompilerParams(
            collective_id=0, has_side_effects=True, vmem_limit_bytes=60 * 1024 * 1024
        ),
        cost_estimate=pl.CostEstimate(flops=flops, bytes_accessed=flops // all_rows, transcendentals=0),
    )(
        tokens,
        lengths,
        cache_key,
        cache_value,
        routes,
        route_logits,
        mix_gain.reshape(1, -1),
        query_gain.reshape(1, -1),
        key_gain.reshape(1, -1),
        head_bias.reshape(-1, 1),
        w_query,
        w_key,
        w_value,
        w_out,
        ffn_gain.reshape(1, -1),
        w_gate,
        w_up,
        w_down,
    )


def solution(mesh):
    n = mesh.shape["ep"]

    def body(*arrays):
        tokens, w_gate = arrays[0], arrays[15]
        share = tokens.shape[1] // n
        if share == 128 and w_gate.shape[1] % COLUMNS == 0:
            return local(n, *arrays)
        return plain(*arrays)

    return jax.shard_map(
        body,
        mesh=mesh,
        in_specs=(
            P(("grp", "ep"), None),
            P(("grp", "ep")),
            P(("grp", "ep"), None, None),
            P(("grp", "ep"), None, None),
            P(("grp", "ep"), None),
            P(("grp", "ep"), None),
            P(),
            P(),
            P(),
            P(),
            P("ep", None),
            P("ep", None),
            P("ep", None),
            P(None, "ep"),
            P(),
            P(None, "ep"),
            P(None, "ep"),
            P("ep", None),
        ),
        out_specs=(P(("grp", "ep"), None), P(("grp", "ep"), None), P(("grp", "ep"), None)),
        check_vma=False,
    )
```

```python
import functools

import jax
import jax.numpy as jnp
from jax import lax
from jax.experimental import pallas as pl
from jax.experimental.pallas import tpu as pltpu
from jax.sharding import PartitionSpec as P

HEADS = 16
KV_HEADS = 4
HEAD_DIM = 64
FF = 7168
EXPERTS = 4


EPSILON = 1e-06


def rms_scaled(values, gain):
    return values * lax.rsqrt(jnp.mean(values * values, axis=-1, keepdims=True) + EPSILON) * gain


def route_weights(routes, route_logits):
    experts_iota = jnp.arange(EXPERTS, dtype=jnp.int32)[None, :]
    first_share = jax.nn.sigmoid(route_logits[:, 0:1] - route_logits[:, 1:2])
    second_share = jax.nn.sigmoid(route_logits[:, 1:2] - route_logits[:, 0:1])
    return jnp.where(routes[:, 0:1] == experts_iota, first_share, 0.0) + jnp.where(
        routes[:, 1:2] == experts_iota, second_share, 0.0
    )


def stick_attend(queries, lengths, cache_key, cache_value, query_gain, head_bias):
    batch_rows = queries.shape[0]
    cache_len = cache_key.shape[1]
    group_size = HEADS // KV_HEADS
    normed_query = rms_scaled(queries.reshape(batch_rows, HEADS, HEAD_DIM), query_gain).astype(
        jnp.bfloat16
    )
    normed_query = normed_query.reshape(batch_rows, KV_HEADS, group_size, HEAD_DIM)
    key_heads = cache_key.reshape(batch_rows, cache_len, KV_HEADS, HEAD_DIM)
    value_heads = cache_value.reshape(batch_rows, cache_len, KV_HEADS, HEAD_DIM)
    scores = jnp.einsum(
        "bkgd,blkd->bkgl", normed_query, key_heads, preferred_element_type=jnp.float32
    ) * HEAD_DIM ** (-0.5)
    scores = scores + head_bias.reshape(KV_HEADS, group_size)[None, :, :, None]
    live_mask = (
        jnp.arange(cache_len, dtype=jnp.int32)[None, None, None, :] < lengths[:, None, None, None]
    )
    remain = jnp.where(live_mask, jax.nn.log_sigmoid(-scores), 0.0)
    after_sum = lax.cumsum(remain, axis=3, reverse=True) - remain
    weights = jnp.where(live_mask, jnp.exp(jax.nn.log_sigmoid(scores) + after_sum), 0.0).astype(
        jnp.bfloat16
    )
    attended = jnp.einsum(
        "bkgl,blkd->bkgd", weights, value_heads, preferred_element_type=jnp.float32
    )
    return attended.reshape(batch_rows, HEADS * HEAD_DIM).astype(jnp.bfloat16)


def plain(
    tokens,
    lengths,
    cache_key,
    cache_value,
    routes,
    route_logits,
    mix_gain,
    query_gain,
    key_gain,
    head_bias,
    w_query,
    w_key,
    w_value,
    w_out,
    ffn_gain,
    w_gate,
    w_up,
    w_down,
):
    token_rows = tokens.shape[0]
    key_width = w_key.shape[1]
    as_float = tokens.astype(jnp.float32)
    normed = rms_scaled(as_float, mix_gain).astype(jnp.bfloat16)
    pieces = (
        lax.all_gather(w_query, "ep", axis=0, tiled=True),
        lax.all_gather(w_key, "ep", axis=0, tiled=True),
        lax.all_gather(w_value, "ep", axis=0, tiled=True),
    )
    queries, fresh_key, fresh_value = tuple(
        (jnp.dot(normed, weight, preferred_element_type=jnp.float32) for weight in pieces)
    )
    new_key = rms_scaled(fresh_key.reshape(token_rows, KV_HEADS, HEAD_DIM), key_gain)
    new_key = new_key.reshape(token_rows, key_width).astype(jnp.bfloat16)
    new_value = fresh_value.astype(jnp.bfloat16)
    attended = stick_attend(queries, lengths, cache_key, cache_value, query_gain, head_bias)
    mixed = as_float + jnp.dot(
        attended,
        lax.all_gather(w_out, "ep", axis=1, tiled=True),
        preferred_element_type=jnp.float32,
    )
    expert_in = rms_scaled(mixed, ffn_gain).astype(jnp.bfloat16)
    every_gate = lax.all_gather(route_weights(routes, route_logits), "ep", axis=0, tiled=True)
    ff_share = w_gate.shape[1]
    my_expert = lax.axis_index("ep") // (FF // ff_share)
    my_gate = lax.dynamic_slice_in_dim(every_gate, my_expert, 1, 1)
    input_rows = lax.all_gather(expert_in, "ep", axis=0, tiled=True)
    gate_value = jnp.dot(input_rows, w_gate, preferred_element_type=jnp.float32)
    up_value = jnp.dot(input_rows, w_up, preferred_element_type=jnp.float32)
    hidden = (jax.nn.silu(gate_value) * up_value * my_gate).astype(jnp.bfloat16)
    expert_sum = lax.psum_scatter(
        jnp.dot(hidden, w_down, preferred_element_type=jnp.float32),
        "ep",
        scatter_dimension=0,
        tiled=True,
    )
    return ((mixed + expert_sum).astype(jnp.bfloat16), new_key, new_value)


WEIGHT_PARTS = 2
DOWN_PARTS = 4
COLUMNS = 256


def dot(left, right):
    return jnp.dot(left, right, preferred_element_type=jnp.float32)


def iota(shape, dim):
    return lax.broadcasted_iota(jnp.int32, shape, dim)


def column(row):
    square = (row.shape[1], row.shape[1])
    return jnp.sum(
        jnp.where(iota(square, 0) == iota(square, 1), jnp.broadcast_to(row, square), 0.0),
        axis=1,
        keepdims=True,
    )


def fused(
    n,
    tokens_hbm,
    lengths_ref,
    ck_hbm,
    cv_hbm,
    routes_hbm,
    logits_hbm,
    mix_gain_hbm,
    query_gain_hbm,
    key_gain_hbm,
    head_bias_hbm,
    wq_hbm,
    wk_hbm,
    wv_hbm,
    wo_hbm,
    ffn_gain_hbm,
    wg_hbm,
    wu_hbm,
    wd_hbm,
    out_any,
    new_key_any,
    new_value_any,
    tokens_ref,
    routes_ref,
    logits_ref,
    mix_gain_ref,
    query_gain_ref,
    key_gain_ref,
    head_bias_ref,
    ffn_gain_ref,
    out_ref,
    new_key_ref,
    new_value_ref,
    wq,
    wk,
    wv,
    wo,
    ck,
    cv,
    wg,
    wu,
    wd,
    s1,
    r1,
    s2,
    r2,
    r3,
    r4,
    s5,
    p5,
    t5,
    r5,
    token_cols,
    aux_rows,
    attended_rows,
    expert_in,
    hidden,
    operand_sem,
    result_sem,
    small_sem,
    key_sem,
    value_sem,
    weight_sem,
    send_sem,
    recv_sem,
    block_sem,
    pair_send_sem,
    pair_sem,
):
    me = lax.axis_index("ep")
    rows, width = tokens_ref.shape
    all_rows = rows * n
    share = width // n
    q_width = wq.shape[1]
    k_width = wk.shape[1]
    cache_len = ck.shape[1]
    group_size = HEADS // KV_HEADS
    ff_share = wg.shape[1]
    my_expert = me // (FF // ff_share)

    barrier = pltpu.get_barrier_semaphore()
    peer_at = [me]
    for d in range(1, n):
        bit = d.bit_length() - 1
        flip = 2**bit * (1 - 2 * ((me // 2**bit) % 2))
        peer_at.append(peer_at[d - 2**bit] + flip)
    furthest_first = range(n - 1, 0, -1)
    core, chip = me % 2, me // 2
    for d in furthest_first:
        pl.semaphore_signal(
            barrier,
            inc=1,
            device_id={"ep": peer_at[d]},
            device_id_type=pl.DeviceIdType.MESH,
        )

    operands = [
        pltpu.make_async_copy(a, b, operand_sem.at[i])
        for i, (a, b) in enumerate(
            (
                (tokens_hbm, tokens_ref),
                (routes_hbm, routes_ref),
                (logits_hbm, logits_ref),
                (mix_gain_hbm, mix_gain_ref),
                (query_gain_hbm, query_gain_ref),
                (key_gain_hbm, key_gain_ref),
                (head_bias_hbm, head_bias_ref),
                (ffn_gain_hbm, ffn_gain_ref),
            )
        )
    ]
    for c in operands:
        c.start()

    small = [
        pltpu.make_async_copy(a, b, small_sem.at[i])
        for i, (a, b) in enumerate(((wq_hbm, wq), (wk_hbm, wk), (wv_hbm, wv), (wo_hbm, wo)))
    ]
    for c in small[:3]:
        c.start()
    keys = [pltpu.make_async_copy(ck_hbm.at[b], ck.at[b], key_sem.at[b]) for b in range(rows)]
    values = [pltpu.make_async_copy(cv_hbm.at[b], cv.at[b], value_sem.at[b]) for b in range(rows)]
    weights = []
    for which, (a, b) in enumerate(((wg_hbm, wg), (wu_hbm, wu), (wd_hbm, wd))):
        step = b.shape[0] // WEIGHT_PARTS
        for part in range(WEIGHT_PARTS):
            piece = pl.ds(part * step, step)
            weights.append(
                pltpu.make_async_copy(
                    a.at[piece], b.at[piece], weight_sem.at[which, part]
                )
            )

    results = [
        pltpu.make_async_copy(a, b, result_sem.at[i])
        for i, (a, b) in enumerate(
            ((out_ref, out_any), (new_key_ref, new_key_any), (new_value_ref, new_value_any))
        )
    ]
    for c in operands:
        c.wait()


    def send(stage, d, source, target, arrival=None):
        copy = pltpu.make_async_remote_copy(
            src_ref=source,
            dst_ref=target,
            send_sem=send_sem.at[stage],
            recv_sem=recv_sem.at[stage] if arrival is None else arrival,
            device_id={"ep": peer_at[d]},
            device_id_type=pl.DeviceIdType.MESH,
        )
        copy.start()

    def arrived(sem, blocks):
        pltpu.make_async_copy(blocks, blocks, sem).wait()

    others = pl.ds(0, n - 1)
    other_chips = pl.ds(0, n // 2 - 1)

    as_float = tokens_ref[...].astype(jnp.float32)
    scale = lax.rsqrt(jnp.mean(as_float * as_float, axis=1, keepdims=True) + EPSILON)
    lane = iota((rows, 128), 1)
    logit_gap = column(logits_ref[0:1] - logits_ref[1:2])
    chosen = [column(routes_ref[i : i + 1].astype(jnp.float32)) for i in range(2)]
    first_share = 1.0 / (1.0 + jnp.exp(-logit_gap))
    second_share = 1.0 / (1.0 + jnp.exp(logit_gap))
    expert_lane = (lane % EXPERTS).astype(jnp.float32)
    gates = jnp.where(chosen[0] == expert_lane, first_share, 0.0) + jnp.where(
        chosen[1] == expert_lane, second_share, 0.0
    )
    aux = jnp.where(lane < 3 * EXPERTS, gates, scale)
    high = aux.astype(jnp.bfloat16).astype(jnp.float32)
    middle = (aux - high).astype(jnp.bfloat16).astype(jnp.float32)
    low = aux - high - middle
    term = jnp.where(lane < 3 * EXPERTS, lane // EXPERTS, lane - 3 * EXPERTS)
    aux = jnp.where(term == 0, high, jnp.where(term == 1, middle, low))
    for peer in range(n):
        block = jnp.concatenate(
            [as_float[:, peer * share : (peer + 1) * share], aux], axis=0
        ).astype(jnp.bfloat16)
        s1[peer] = block
    pl.semaphore_wait(barrier, n - 1)
    for d in furthest_first:
        send(0, d, s1.at[peer_at[d]], r1.at[me])
    for c in keys + values + small[3:]:
        c.start()
    r1[me] = s1[me]
    for c in small[:3]:
        c.wait()
    arrived(recv_sem.at[0], r1.at[others])
    for c in weights:
        c.start()
    for peer in range(n):
        block = r1[peer].astype(jnp.float32)
        token_cols[peer * rows : (peer + 1) * rows, :] = block[:rows]
        aux_rows[peer * rows : (peer + 1) * rows, :] = block[rows:]
    aux = aux_rows[...]
    lane = iota(aux.shape, 1)
    row_scale = jnp.sum(
        jnp.where((lane >= 3 * EXPERTS) & (lane < 3 * EXPERTS + 3), aux, 0.0), axis=1, keepdims=True
    )
    my_gate = jnp.sum(
        jnp.where((lane < 3 * EXPERTS) & (lane % EXPERTS == my_expert), aux, 0.0),
        axis=1,
        keepdims=True,
    )
    my_gain = mix_gain_ref[:, pl.ds(pl.multiple_of(me * share, share), share)]
    normed = (token_cols[...] * row_scale * my_gain).astype(jnp.bfloat16)

    for weight, start in ((wq, 0), (wk, q_width), (wv, q_width + k_width)):
        partial = dot(normed, weight[...])
        for peer in range(n):
            s2[peer, :, start : start + weight.shape[1]] = partial[
                peer * rows : (peer + 1) * rows
            ].astype(jnp.bfloat16)
    for d in furthest_first:
        send(1, d, s2.at[peer_at[d]], r2.at[me])
    r2[me] = s2[me]

    head_of_lane = iota((HEADS, q_width), 1) // HEAD_DIM
    own_lane = head_of_lane == iota((HEADS, q_width), 0)
    source_lane = iota((q_width, k_width), 0)
    target_lane = iota((q_width, k_width), 1)
    fold = jnp.where(
        (source_lane // (HEAD_DIM * group_size) == target_lane // HEAD_DIM)
        & (source_lane % HEAD_DIM == target_lane % HEAD_DIM),
        1.0,
        0.0,
    ).astype(jnp.bfloat16)
    later = jnp.where(
        iota((COLUMNS, COLUMNS), 0) > iota((COLUMNS, COLUMNS), 1), 1.0, 0.0
    ).astype(jnp.bfloat16)
    query_gain = jnp.concatenate([query_gain_ref[...]] * HEADS, axis=1)
    key_gain = jnp.concatenate([key_gain_ref[...]] * KV_HEADS, axis=1)

    arrived(recv_sem.at[1], r2.at[others])
    total = r2[0].astype(jnp.float32)
    for peer in range(1, n):
        total = total + r2[peer].astype(jnp.float32)
    queries = total[:, :q_width]
    fresh_key = total[:, q_width : q_width + k_width]
    new_value_ref[...] = total[:, q_width + k_width :].astype(jnp.bfloat16)
    squares = fresh_key * fresh_key
    key_lane = iota(squares.shape, 1) // HEAD_DIM
    key_scale = jnp.zeros_like(squares)
    for g in range(KV_HEADS):
        mean = jnp.sum(jnp.where(key_lane == g, squares, 0.0), axis=1, keepdims=True) / HEAD_DIM
        key_scale = jnp.where(key_lane == g, lax.rsqrt(mean + EPSILON), key_scale)
    new_key_ref[...] = (fresh_key * key_scale * key_gain).astype(jnp.bfloat16)

    for c in results[1:]:
        c.start()

    spread = []
    for b in range(rows):
        wide = jnp.where(own_lane, jnp.broadcast_to(queries[b : b + 1], own_lane.shape), 0.0)
        mean = jnp.sum(wide * wide, axis=1, keepdims=True) / HEAD_DIM
        spread.append((wide * lax.rsqrt(mean + EPSILON) * query_gain).astype(jnp.bfloat16))
    folded = dot(jnp.concatenate(spread, axis=0), fold).astype(jnp.bfloat16)
    blocks = cache_len // COLUMNS
    position = iota((HEADS, cache_len), 1)
    own_group = iota((HEADS, k_width), 1) // HEAD_DIM == iota((HEADS, k_width), 0) // group_size
    head_bias = column(head_bias_ref[...])
    heads = []
    for b in range(rows):
        keys[b].wait()
        scores = lax.dot_general(
            folded[b * HEADS : (b + 1) * HEADS],
            ck[b],
            (((1,), (1,)), ((), ())),
            preferred_element_type=jnp.float32,
        ) * HEAD_DIM ** (-0.5)
        scores = scores + head_bias
        live = position < lengths_ref[b]
        tail_log = jnp.log1p(jnp.exp(-jnp.abs(scores)))
        remain = jnp.where(live, jnp.minimum(-scores, 0.0) - tail_log, 0.0)
        stacked = jnp.concatenate(
            [remain[:, i * COLUMNS : (i + 1) * COLUMNS] for i in range(blocks)], axis=0
        )
        high = stacked.astype(jnp.bfloat16)
        rest = stacked - high.astype(jnp.float32)
        middle = rest.astype(jnp.bfloat16)
        low = (rest - middle.astype(jnp.float32)).astype(jnp.bfloat16)
        sums = dot(jnp.concatenate([high, middle, low], axis=0), later)
        count = blocks * HEADS
        sums = sums[:count] + sums[count : 2 * count] + sums[2 * count :]
        totals = jnp.sum(stacked, axis=1, keepdims=True)
        after = [None] * blocks
        carry = jnp.zeros((HEADS, 1), jnp.float32)
        for i in reversed(range(blocks)):
            after[i] = sums[i * HEADS : (i + 1) * HEADS] + carry
            carry = carry + totals[i * HEADS : (i + 1) * HEADS]
        after_sum = jnp.concatenate(after, axis=1)
        chance = jnp.exp(jnp.minimum(scores, 0.0) - tail_log + after_sum)
        weight = jnp.where(live, chance, 0.0).astype(jnp.bfloat16)
        values[b].wait()
        mixed_heads = dot(weight, cv[b])
        heads.append(jnp.where(own_group, mixed_heads, 0.0).astype(jnp.bfloat16))
    unfolded = lax.dot_general(
        jnp.concatenate(heads, axis=0),
        fold,
        (((1,), (1,)), ((), ())),
        preferred_element_type=jnp.float32,
    )
    attended = [
        jnp.sum(
            jnp.where(own_lane, unfolded[b * HEADS : (b + 1) * HEADS], 0.0), axis=0, keepdims=True
        )
        for b in range(rows)
    ]
    r3[me] = jnp.concatenate(attended, axis=0).astype(jnp.bfloat16)

    for d in furthest_first:
        send(2, d, r3.at[me], r3.at[me])
    small[3].wait()
    arrived(recv_sem.at[2], r3.at[others])
    for peer in range(n):
        attended_rows[peer * rows : (peer + 1) * rows, :] = r3[peer].astype(jnp.float32)
    mixed = token_cols[...] + dot(attended_rows[...].astype(jnp.bfloat16), wo[...])
    r4[me] = mixed.astype(jnp.bfloat16)

    for d in range(n - 2, 0, -2):
        send(3, d, r4.at[me], r4.at[me], block_sem.at[me])
    send(3, 1, r4.at[me], r4.at[me], block_sem.at[me])
    for d in range(2, n, 2):
        source = peer_at[d]
        arrived(block_sem.at[source], r4.at[source])
        send(3, 1, r4.at[source], r4.at[source], block_sem.at[source])
    for d in range(1, n, 2):
        source = peer_at[d]
        arrived(block_sem.at[source], r4.at[source])
    squares = jnp.zeros((all_rows, share), jnp.float32)
    for peer in range(n):
        block = r4[peer].astype(jnp.float32)
        squares = squares + block * block
    scale = lax.rsqrt(jnp.sum(squares, axis=1, keepdims=True) / width + EPSILON)
    pick = jnp.where(
        iota((8, all_rows), 1) == iota((8, all_rows), 0) + me * rows, 1.0, 0.0
    ).astype(jnp.bfloat16)
    own_mixed = []
    for peer in range(n):
        columns = slice(peer * share, (peer + 1) * share)
        block = r4[peer]
        own_mixed.append(dot(pick, block)[:rows])
        expert_in[:, columns] = (
            block.astype(jnp.float32) * scale * ffn_gain_ref[:, columns]
        ).astype(jnp.bfloat16)
    own_mixed = jnp.concatenate(own_mixed, axis=1)

    for c in weights[: 2 * WEIGHT_PARTS]:
        c.wait()

    def hidden_step(i, carry):
        columns = pl.ds(pl.multiple_of(i * COLUMNS, COLUMNS), COLUMNS)
        gate_value = dot(expert_in[...], wg[:, columns])
        up_value = dot(expert_in[...], wu[:, columns])
        silu = gate_value / (1.0 + jnp.exp(-gate_value))
        hidden[:, columns] = (silu * up_value * my_gate).astype(jnp.bfloat16)
        return carry

    lax.fori_loop(0, ff_share // COLUMNS, hidden_step, 0)

    for c in weights[2 * WEIGHT_PARTS :]:
        c.wait()

    step = width // DOWN_PARTS

    pairs = []

    def spread_sums(part):
        arrived(pair_sem.at[part], p5.at[part])
        both = s5[part, core].astype(jnp.float32) + p5[part].astype(jnp.float32)
        t5[part] = both.astype(jnp.bfloat16)
        for d in range(n - 2, 0, -2):
            send(4 + part, d, t5.at[part, peer_at[d] // 2], r5.at[part, chip])
        r5[part, chip] = t5[part, chip]

    for part in range(DOWN_PARTS):
        partial = dot(hidden[...], wd[:, part * step : (part + 1) * step])
        for peer in range(n):
            s5[part, peer % 2, peer // 2] = partial[peer * rows : (peer + 1) * rows].astype(
                jnp.bfloat16
            )
        pairs.append(
            pltpu.make_async_remote_copy(
                src_ref=s5.at[part, 1 - core],
                dst_ref=p5.at[part],
                send_sem=pair_send_sem.at[part],
                recv_sem=pair_sem.at[part],
                device_id={"ep": peer_at[1]},
                device_id_type=pl.DeviceIdType.MESH,
            )
        )
        pairs[-1].start()
        if part:
            spread_sums(part - 1)
    spread_sums(DOWN_PARTS - 1)
    for part in range(DOWN_PARTS):
        arrived(recv_sem.at[4 + part], r5.at[part, other_chips])
        total = own_mixed[:, part * step : (part + 1) * step]
        for peer in range(n // 2):
            total = total + r5[part, peer].astype(jnp.float32)
        out_ref[:, part * step : (part + 1) * step] = total.astype(jnp.bfloat16)
    results[0].start()
    for stage, blocks in enumerate((s1, s2, r3, r4)):
        arrived(send_sem.at[stage], blocks.at[others])
    for part in range(DOWN_PARTS):
        pairs[part].wait_send()
        arrived(send_sem.at[4 + part], t5.at[part, other_chips])
    for c in results:
        c.wait()


def local(
    n,
    tokens,
    lengths,
    cache_key,
    cache_value,
    routes,
    route_logits,
    mix_gain,
    query_gain,
    key_gain,
    head_bias,
    w_query,
    w_key,
    w_value,
    w_out,
    ffn_gain,
    w_gate,
    w_up,
    w_down,
):
    rows, width = tokens.shape
    all_rows = rows * n
    share = width // n
    q_width, k_width = w_query.shape[1], w_key.shape[1]
    wide = q_width + k_width + w_value.shape[1]
    stages = 4 + DOWN_PARTS
    anywhere = pl.BlockSpec(memory_space=pl.ANY)
    smem = pl.BlockSpec(memory_space=pltpu.SMEM)
    bf16, f32 = jnp.bfloat16, jnp.float32

    def like(array):
        return pltpu.VMEM(array.shape, array.dtype)

    flops = 2 * all_rows * 3 * w_gate.shape[0] * w_gate.shape[1]
    shapes = ((rows, width), (rows, k_width), (rows, w_value.shape[1]))
    return pl.pallas_call(
        functools.partial(fused, n),
        out_shape=tuple(pltpu.VMEM(shape, bf16) for shape in shapes),
        in_specs=[anywhere, smem] + [anywhere] * 16,
        out_specs=(anywhere,) * 3,
        scratch_shapes=[
            like(tokens),
            pltpu.VMEM(routes.shape[::-1], routes.dtype),
            pltpu.VMEM(route_logits.shape[::-1], f32),
            pltpu.VMEM((1, width), f32),
            pltpu.VMEM((1, HEAD_DIM), f32),
            pltpu.VMEM((1, HEAD_DIM), f32),
            pltpu.VMEM((1, HEADS), f32),
            pltpu.VMEM((1, width), f32),
            *(pltpu.VMEM(shape, bf16) for shape in shapes),
            like(w_query),
            like(w_key),
            like(w_value),
            like(w_out),
            like(cache_key),
            like(cache_value),
            like(w_gate),
            like(w_up),
            like(w_down),
            pltpu.VMEM((n, 2 * rows, share), bf16),
            pltpu.VMEM((n, 2 * rows, share), bf16),
            pltpu.VMEM((n, rows, wide), bf16),
            pltpu.VMEM((n, rows, wide), bf16),
            pltpu.VMEM((n, rows, q_width), bf16),
            pltpu.VMEM((n, all_rows, share), bf16),
            pltpu.VMEM((DOWN_PARTS, 2, n // 2, rows, width // DOWN_PARTS), bf16),
            pltpu.VMEM((DOWN_PARTS, n // 2, rows, width // DOWN_PARTS), bf16),
            pltpu.VMEM((DOWN_PARTS, n // 2, rows, width // DOWN_PARTS), bf16),
            pltpu.VMEM((DOWN_PARTS, n // 2, rows, width // DOWN_PARTS), bf16),
            pltpu.VMEM((all_rows, share), f32),
            pltpu.VMEM((all_rows, share), f32),
            pltpu.VMEM((all_rows, q_width), f32),
            pltpu.VMEM((all_rows, width), bf16),
            pltpu.VMEM((all_rows, w_gate.shape[1]), bf16),
            pltpu.SemaphoreType.DMA((8,)),
            pltpu.SemaphoreType.DMA((3,)),
            pltpu.SemaphoreType.DMA((4,)),
            pltpu.SemaphoreType.DMA((rows,)),
            pltpu.SemaphoreType.DMA((rows,)),
            pltpu.SemaphoreType.DMA((3, WEIGHT_PARTS)),
            pltpu.SemaphoreType.DMA((stages,)),
            pltpu.SemaphoreType.DMA((stages,)),
            pltpu.SemaphoreType.DMA((n,)),
            pltpu.SemaphoreType.DMA((DOWN_PARTS,)),
            pltpu.SemaphoreType.DMA((DOWN_PARTS,)),
        ],
        compiler_params=pltpu.CompilerParams(
            collective_id=0, has_side_effects=True, vmem_limit_bytes=60 * 1024 * 1024
        ),
        cost_estimate=pl.CostEstimate(flops=flops, bytes_accessed=flops // all_rows, transcendentals=0),
    )(
        tokens,
        lengths,
        cache_key,
        cache_value,
        routes.T,
        route_logits.T,
        mix_gain.reshape(1, -1),
        query_gain.reshape(1, -1),
        key_gain.reshape(1, -1),
        head_bias.reshape(1, -1),
        w_query,
        w_key,
        w_value,
        w_out,
        ffn_gain.reshape(1, -1),
        w_gate,
        w_up,
        w_down,
    )


def solution(mesh):
    n = mesh.shape["ep"]

    def body(*arrays):
        tokens, w_gate = arrays[0], arrays[15]
        share = tokens.shape[1] // n
        if share == 128 and n & (n - 1) == 0 and w_gate.shape[1] % COLUMNS == 0:
            return local(n, *arrays)
        return plain(*arrays)

    return jax.shard_map(
        body,
        mesh=mesh,
        in_specs=(
            P(("grp", "ep"), None),
            P(("grp", "ep")),
            P(("grp", "ep"), None, None),
            P(("grp", "ep"), None, None),
            P(("grp", "ep"), None),
            P(("grp", "ep"), None),
            P(),
            P(),
            P(),
            P(),
            P("ep", None),
            P("ep", None),
            P("ep", None),
            P(None, "ep"),
            P(),
            P(None, "ep"),
            P(None, "ep"),
            P("ep", None),
        ),
        out_specs=(P(("grp", "ep"), None), P(("grp", "ep"), None), P(("grp", "ep"), None)),
        check_vma=False,
    )
```

```python
import functools

import jax
import jax.numpy as jnp
from jax import lax
from jax.experimental import pallas as pl
from jax.experimental.pallas import tpu as pltpu
from jax.sharding import PartitionSpec as P

HEADS = 16
KV_HEADS = 4
HEAD_DIM = 64
FF = 7168
EXPERTS = 4


EPSILON = 1e-06


def rms_scaled(values, gain):
    return values * lax.rsqrt(jnp.mean(values * values, axis=-1, keepdims=True) + EPSILON) * gain


def route_weights(routes, route_logits):
    experts_iota = jnp.arange(EXPERTS, dtype=jnp.int32)[None, :]
    first_share = jax.nn.sigmoid(route_logits[:, 0:1] - route_logits[:, 1:2])
    second_share = jax.nn.sigmoid(route_logits[:, 1:2] - route_logits[:, 0:1])
    return jnp.where(routes[:, 0:1] == experts_iota, first_share, 0.0) + jnp.where(
        routes[:, 1:2] == experts_iota, second_share, 0.0
    )


def stick_attend(queries, lengths, cache_key, cache_value, query_gain, head_bias):
    batch_rows = queries.shape[0]
    cache_len = cache_key.shape[1]
    group_size = HEADS // KV_HEADS
    normed_query = rms_scaled(queries.reshape(batch_rows, HEADS, HEAD_DIM), query_gain).astype(
        jnp.bfloat16
    )
    normed_query = normed_query.reshape(batch_rows, KV_HEADS, group_size, HEAD_DIM)
    key_heads = cache_key.reshape(batch_rows, cache_len, KV_HEADS, HEAD_DIM)
    value_heads = cache_value.reshape(batch_rows, cache_len, KV_HEADS, HEAD_DIM)
    scores = jnp.einsum(
        "bkgd,blkd->bkgl", normed_query, key_heads, preferred_element_type=jnp.float32
    ) * HEAD_DIM ** (-0.5)
    scores = scores + head_bias.reshape(KV_HEADS, group_size)[None, :, :, None]
    live_mask = (
        jnp.arange(cache_len, dtype=jnp.int32)[None, None, None, :] < lengths[:, None, None, None]
    )
    remain = jnp.where(live_mask, jax.nn.log_sigmoid(-scores), 0.0)
    after_sum = lax.cumsum(remain, axis=3, reverse=True) - remain
    weights = jnp.where(live_mask, jnp.exp(jax.nn.log_sigmoid(scores) + after_sum), 0.0).astype(
        jnp.bfloat16
    )
    attended = jnp.einsum(
        "bkgl,blkd->bkgd", weights, value_heads, preferred_element_type=jnp.float32
    )
    return attended.reshape(batch_rows, HEADS * HEAD_DIM).astype(jnp.bfloat16)


def plain(
    tokens,
    lengths,
    cache_key,
    cache_value,
    routes,
    route_logits,
    mix_gain,
    query_gain,
    key_gain,
    head_bias,
    w_query,
    w_key,
    w_value,
    w_out,
    ffn_gain,
    w_gate,
    w_up,
    w_down,
):
    token_rows = tokens.shape[0]
    key_width = w_key.shape[1]
    as_float = tokens.astype(jnp.float32)
    normed = rms_scaled(as_float, mix_gain).astype(jnp.bfloat16)
    pieces = (
        lax.all_gather(w_query, "ep", axis=0, tiled=True),
        lax.all_gather(w_key, "ep", axis=0, tiled=True),
        lax.all_gather(w_value, "ep", axis=0, tiled=True),
    )
    queries, fresh_key, fresh_value = tuple(
        (jnp.dot(normed, weight, preferred_element_type=jnp.float32) for weight in pieces)
    )
    new_key = rms_scaled(fresh_key.reshape(token_rows, KV_HEADS, HEAD_DIM), key_gain)
    new_key = new_key.reshape(token_rows, key_width).astype(jnp.bfloat16)
    new_value = fresh_value.astype(jnp.bfloat16)
    attended = stick_attend(queries, lengths, cache_key, cache_value, query_gain, head_bias)
    mixed = as_float + jnp.dot(
        attended,
        lax.all_gather(w_out, "ep", axis=1, tiled=True),
        preferred_element_type=jnp.float32,
    )
    expert_in = rms_scaled(mixed, ffn_gain).astype(jnp.bfloat16)
    every_gate = lax.all_gather(route_weights(routes, route_logits), "ep", axis=0, tiled=True)
    ff_share = w_gate.shape[1]
    my_expert = lax.axis_index("ep") // (FF // ff_share)
    my_gate = lax.dynamic_slice_in_dim(every_gate, my_expert, 1, 1)
    input_rows = lax.all_gather(expert_in, "ep", axis=0, tiled=True)
    gate_value = jnp.dot(input_rows, w_gate, preferred_element_type=jnp.float32)
    up_value = jnp.dot(input_rows, w_up, preferred_element_type=jnp.float32)
    hidden = (jax.nn.silu(gate_value) * up_value * my_gate).astype(jnp.bfloat16)
    expert_sum = lax.psum_scatter(
        jnp.dot(hidden, w_down, preferred_element_type=jnp.float32),
        "ep",
        scatter_dimension=0,
        tiled=True,
    )
    return ((mixed + expert_sum).astype(jnp.bfloat16), new_key, new_value)


WEIGHT_PARTS = 2
DOWN_PARTS = 4
COLUMNS = 256


def dot(left, right):
    return jnp.dot(left, right, preferred_element_type=jnp.float32)


def iota(shape, dim):
    return lax.broadcasted_iota(jnp.int32, shape, dim)


def column(row):
    square = (row.shape[1], row.shape[1])
    return jnp.sum(
        jnp.where(iota(square, 0) == iota(square, 1), jnp.broadcast_to(row, square), 0.0),
        axis=1,
        keepdims=True,
    )


def fused(
    n,
    tokens_hbm,
    lengths_ref,
    ck_hbm,
    cv_hbm,
    routes_hbm,
    logits_hbm,
    mix_gain_hbm,
    query_gain_hbm,
    key_gain_hbm,
    head_bias_hbm,
    wq_hbm,
    wk_hbm,
    wv_hbm,
    wo_hbm,
    ffn_gain_hbm,
    wg_hbm,
    wu_hbm,
    wd_hbm,
    out_any,
    new_key_any,
    new_value_any,
    tokens_ref,
    routes_ref,
    logits_ref,
    mix_gain_ref,
    query_gain_ref,
    key_gain_ref,
    head_bias_ref,
    ffn_gain_ref,
    out_ref,
    new_key_ref,
    new_value_ref,
    wq,
    wk,
    wv,
    wo,
    ck,
    cv,
    wg,
    wu,
    wd,
    s1,
    r1,
    s2,
    p2,
    t2,
    r2,
    r3,
    r4,
    s5,
    p5,
    t5,
    r5,
    token_cols,
    aux_rows,
    attended_rows,
    expert_in,
    hidden,
    operand_sem,
    result_sem,
    small_sem,
    key_sem,
    value_sem,
    weight_sem,
    send_sem,
    recv_sem,
    block_sem,
    pair_send_sem,
    pair_sem,
):
    me = lax.axis_index("ep")
    rows, width = tokens_ref.shape
    all_rows = rows * n
    share = width // n
    q_width = wq.shape[1]
    k_width = wk.shape[1]
    cache_len = ck.shape[1]
    group_size = HEADS // KV_HEADS
    ff_share = wg.shape[1]
    my_expert = me // (FF // ff_share)

    barrier = pltpu.get_barrier_semaphore()
    peer_at = [me]
    for d in range(1, n):
        bit = d.bit_length() - 1
        flip = 2**bit * (1 - 2 * ((me // 2**bit) % 2))
        peer_at.append(peer_at[d - 2**bit] + flip)
    furthest_first = range(n - 1, 0, -1)
    core, chip = me % 2, me // 2
    for d in furthest_first:
        pl.semaphore_signal(
            barrier,
            inc=1,
            device_id={"ep": peer_at[d]},
            device_id_type=pl.DeviceIdType.MESH,
        )

    operands = [
        pltpu.make_async_copy(a, b, operand_sem.at[i])
        for i, (a, b) in enumerate(
            (
                (tokens_hbm, tokens_ref),
                (routes_hbm, routes_ref),
                (logits_hbm, logits_ref),
                (mix_gain_hbm, mix_gain_ref),
                (query_gain_hbm, query_gain_ref),
                (key_gain_hbm, key_gain_ref),
                (head_bias_hbm, head_bias_ref),
                (ffn_gain_hbm, ffn_gain_ref),
            )
        )
    ]
    for c in operands:
        c.start()

    small = [
        pltpu.make_async_copy(a, b, small_sem.at[i])
        for i, (a, b) in enumerate(((wq_hbm, wq), (wk_hbm, wk), (wv_hbm, wv), (wo_hbm, wo)))
    ]
    for c in small[:3]:
        c.start()
    keys = [pltpu.make_async_copy(ck_hbm.at[b], ck.at[b], key_sem.at[b]) for b in range(rows)]
    values = [pltpu.make_async_copy(cv_hbm.at[b], cv.at[b], value_sem.at[b]) for b in range(rows)]
    weights = []
    for which, (a, b) in enumerate(((wg_hbm, wg), (wu_hbm, wu), (wd_hbm, wd))):
        step = b.shape[0] // WEIGHT_PARTS
        for part in range(WEIGHT_PARTS):
            piece = pl.ds(part * step, step)
            weights.append(
                pltpu.make_async_copy(
                    a.at[piece], b.at[piece], weight_sem.at[which, part]
                )
            )

    results = [
        pltpu.make_async_copy(a, b, result_sem.at[i])
        for i, (a, b) in enumerate(
            ((out_ref, out_any), (new_key_ref, new_key_any), (new_value_ref, new_value_any))
        )
    ]
    for c in operands:
        c.wait()


    def send(stage, d, source, target, arrival=None):
        copy = pltpu.make_async_remote_copy(
            src_ref=source,
            dst_ref=target,
            send_sem=send_sem.at[stage],
            recv_sem=recv_sem.at[stage] if arrival is None else arrival,
            device_id={"ep": peer_at[d]},
            device_id_type=pl.DeviceIdType.MESH,
        )
        copy.start()

    def arrived(sem, blocks):
        pltpu.make_async_copy(blocks, blocks, sem).wait()

    others = pl.ds(0, n - 1)
    other_chips = pl.ds(0, n // 2 - 1)

    as_float = tokens_ref[...].astype(jnp.float32)
    scale = lax.rsqrt(jnp.mean(as_float * as_float, axis=1, keepdims=True) + EPSILON)
    lane = iota((rows, 128), 1)
    logit_gap = column(logits_ref[0:1] - logits_ref[1:2])
    chosen = [column(routes_ref[i : i + 1].astype(jnp.float32)) for i in range(2)]
    first_share = 1.0 / (1.0 + jnp.exp(-logit_gap))
    second_share = 1.0 / (1.0 + jnp.exp(logit_gap))
    expert_lane = (lane % EXPERTS).astype(jnp.float32)
    gates = jnp.where(chosen[0] == expert_lane, first_share, 0.0) + jnp.where(
        chosen[1] == expert_lane, second_share, 0.0
    )
    aux = jnp.where(lane < 3 * EXPERTS, gates, scale)
    high = aux.astype(jnp.bfloat16).astype(jnp.float32)
    middle = (aux - high).astype(jnp.bfloat16).astype(jnp.float32)
    low = aux - high - middle
    term = jnp.where(lane < 3 * EXPERTS, lane // EXPERTS, lane - 3 * EXPERTS)
    aux = jnp.where(term == 0, high, jnp.where(term == 1, middle, low))
    for peer in range(n):
        block = jnp.concatenate(
            [as_float[:, peer * share : (peer + 1) * share], aux], axis=0
        ).astype(jnp.bfloat16)
        s1[peer] = block
    pl.semaphore_wait(barrier, n - 1)
    for d in furthest_first:
        send(0, d, s1.at[peer_at[d]], r1.at[me])
    for c in keys + values + small[3:]:
        c.start()
    r1[me] = s1[me]
    for c in small[:3]:
        c.wait()
    arrived(recv_sem.at[0], r1.at[others])
    for c in weights:
        c.start()
    for peer in range(n):
        block = r1[peer].astype(jnp.float32)
        token_cols[peer * rows : (peer + 1) * rows, :] = block[:rows]
        aux_rows[peer * rows : (peer + 1) * rows, :] = block[rows:]
    aux = aux_rows[...]
    lane = iota(aux.shape, 1)
    row_scale = jnp.sum(
        jnp.where((lane >= 3 * EXPERTS) & (lane < 3 * EXPERTS + 3), aux, 0.0), axis=1, keepdims=True
    )
    my_gate = jnp.sum(
        jnp.where((lane < 3 * EXPERTS) & (lane % EXPERTS == my_expert), aux, 0.0),
        axis=1,
        keepdims=True,
    )
    my_gain = mix_gain_ref[:, pl.ds(pl.multiple_of(me * share, share), share)]
    normed = (token_cols[...] * row_scale * my_gain).astype(jnp.bfloat16)

    for weight, start in ((wq, 0), (wk, q_width), (wv, q_width + k_width)):
        partial = dot(normed, weight[...])
        for peer in range(n):
            s2[peer % 2, peer // 2, :, start : start + weight.shape[1]] = partial[
                peer * rows : (peer + 1) * rows
            ].astype(jnp.bfloat16)
    pair = pltpu.make_async_remote_copy(
        src_ref=s2.at[1 - core],
        dst_ref=p2,
        send_sem=pair_send_sem.at[DOWN_PARTS],
        recv_sem=pair_sem.at[DOWN_PARTS],
        device_id={"ep": peer_at[1]},
        device_id_type=pl.DeviceIdType.MESH,
    )
    pair.start()

    head_of_lane = iota((HEADS, q_width), 1) // HEAD_DIM
    own_lane = head_of_lane == iota((HEADS, q_width), 0)
    source_lane = iota((q_width, k_width), 0)
    target_lane = iota((q_width, k_width), 1)
    fold = jnp.where(
        (source_lane // (HEAD_DIM * group_size) == target_lane // HEAD_DIM)
        & (source_lane % HEAD_DIM == target_lane % HEAD_DIM),
        1.0,
        0.0,
    ).astype(jnp.bfloat16)
    later = jnp.where(
        iota((COLUMNS, COLUMNS), 0) > iota((COLUMNS, COLUMNS), 1), 1.0, 0.0
    ).astype(jnp.bfloat16)
    query_gain = jnp.concatenate([query_gain_ref[...]] * HEADS, axis=1)
    key_gain = jnp.concatenate([key_gain_ref[...]] * KV_HEADS, axis=1)

    pair.wait_recv()
    t2[...] = (s2[core].astype(jnp.float32) + p2[...].astype(jnp.float32)).astype(jnp.bfloat16)
    for d in range(n - 2, 0, -2):
        send(1, d, t2.at[peer_at[d] // 2], r2.at[chip])
    r2[chip] = t2[chip]
    arrived(recv_sem.at[1], r2.at[other_chips])
    total = r2[0].astype(jnp.float32)
    for peer in range(1, n // 2):
        total = total + r2[peer].astype(jnp.float32)
    queries = total[:, :q_width]
    fresh_key = total[:, q_width : q_width + k_width]
    new_value_ref[...] = total[:, q_width + k_width :].astype(jnp.bfloat16)
    squares = fresh_key * fresh_key
    key_lane = iota(squares.shape, 1) // HEAD_DIM
    key_scale = jnp.zeros_like(squares)
    for g in range(KV_HEADS):
        mean = jnp.sum(jnp.where(key_lane == g, squares, 0.0), axis=1, keepdims=True) / HEAD_DIM
        key_scale = jnp.where(key_lane == g, lax.rsqrt(mean + EPSILON), key_scale)
    new_key_ref[...] = (fresh_key * key_scale * key_gain).astype(jnp.bfloat16)

    for c in results[1:]:
        c.start()

    spread = []
    for b in range(rows):
        wide = jnp.where(own_lane, jnp.broadcast_to(queries[b : b + 1], own_lane.shape), 0.0)
        mean = jnp.sum(wide * wide, axis=1, keepdims=True) / HEAD_DIM
        spread.append((wide * lax.rsqrt(mean + EPSILON) * query_gain).astype(jnp.bfloat16))
    folded = dot(jnp.concatenate(spread, axis=0), fold).astype(jnp.bfloat16)
    blocks = cache_len // COLUMNS
    head_rows = rows * HEADS
    head_bias = jnp.concatenate([column(head_bias_ref[...])] * rows, axis=0)
    row_of = iota((head_rows, 1), 0) // HEADS
    lengths = jnp.zeros((head_rows, 1), jnp.int32)
    for b in range(rows):
        lengths = jnp.where(row_of == b, lengths_ref[b], lengths)
    live = iota((head_rows, cache_len), 1) < lengths
    for c in keys + values:
        c.wait()
    scores = jnp.concatenate(
        [
            lax.dot_general(
                folded[b * HEADS : (b + 1) * HEADS],
                ck[b],
                (((1,), (1,)), ((), ())),
                preferred_element_type=jnp.float32,
            )
            for b in range(rows)
        ],
        axis=0,
    )
    scores = scores * HEAD_DIM ** (-0.5) + head_bias
    tail_log = jnp.log1p(jnp.exp(-jnp.abs(scores)))
    remain = jnp.where(live, jnp.minimum(-scores, 0.0) - tail_log, 0.0)
    after = [None] * blocks
    carry = jnp.zeros((head_rows, 1), jnp.float32)
    for i in reversed(range(blocks)):
        block = remain[:, i * COLUMNS : (i + 1) * COLUMNS]
        high = block.astype(jnp.bfloat16)
        low = (block - high.astype(jnp.float32)).astype(jnp.bfloat16)
        after[i] = dot(high, later) + dot(low, later) + carry
        carry = carry + jnp.sum(block, axis=1, keepdims=True)
    after_sum = jnp.concatenate(after, axis=1)
    chance = jnp.exp(jnp.minimum(scores, 0.0) - tail_log + after_sum)
    weight = jnp.where(live, chance, 0.0).astype(jnp.bfloat16)
    mixed_heads = jnp.concatenate(
        [dot(weight[b * HEADS : (b + 1) * HEADS], cv[b]) for b in range(rows)], axis=0
    )
    own_group = (
        iota((head_rows, k_width), 1) // HEAD_DIM
        == iota((head_rows, k_width), 0) % HEADS // group_size
    )
    heads = jnp.where(own_group, mixed_heads, 0.0).astype(jnp.bfloat16)
    unfolded = lax.dot_general(
        heads,
        fold,
        (((1,), (1,)), ((), ())),
        preferred_element_type=jnp.float32,
    )
    attended = [
        jnp.sum(
            jnp.where(own_lane, unfolded[b * HEADS : (b + 1) * HEADS], 0.0), axis=0, keepdims=True
        )
        for b in range(rows)
    ]
    r3[me] = jnp.concatenate(attended, axis=0).astype(jnp.bfloat16)

    for d in furthest_first:
        send(2, d, r3.at[me], r3.at[me])
    small[3].wait()
    arrived(recv_sem.at[2], r3.at[others])
    for peer in range(n):
        attended_rows[peer * rows : (peer + 1) * rows, :] = r3[peer].astype(jnp.float32)
    mixed = token_cols[...] + dot(attended_rows[...].astype(jnp.bfloat16), wo[...])
    r4[me] = mixed.astype(jnp.bfloat16)

    for d in range(n - 2, 0, -2):
        send(3, d, r4.at[me], r4.at[me], block_sem.at[me])
    send(3, 1, r4.at[me], r4.at[me], block_sem.at[me])
    for d in range(2, n, 2):
        source = peer_at[d]
        arrived(block_sem.at[source], r4.at[source])
        send(3, 1, r4.at[source], r4.at[source], block_sem.at[source])
    for d in range(1, n, 2):
        source = peer_at[d]
        arrived(block_sem.at[source], r4.at[source])
    squares = jnp.zeros((all_rows, share), jnp.float32)
    for peer in range(n):
        block = r4[peer].astype(jnp.float32)
        squares = squares + block * block
    scale = lax.rsqrt(jnp.sum(squares, axis=1, keepdims=True) / width + EPSILON)
    pick = jnp.where(
        iota((8, all_rows), 1) == iota((8, all_rows), 0) + me * rows, 1.0, 0.0
    ).astype(jnp.bfloat16)
    own_mixed = []
    for peer in range(n):
        columns = slice(peer * share, (peer + 1) * share)
        block = r4[peer]
        own_mixed.append(dot(pick, block)[:rows])
        expert_in[:, columns] = (
            block.astype(jnp.float32) * scale * ffn_gain_ref[:, columns]
        ).astype(jnp.bfloat16)
    own_mixed = jnp.concatenate(own_mixed, axis=1)

    for c in weights[: 2 * WEIGHT_PARTS]:
        c.wait()

    def hidden_step(i, carry):
        columns = pl.ds(pl.multiple_of(i * COLUMNS, COLUMNS), COLUMNS)
        gate_value = dot(expert_in[...], wg[:, columns])
        up_value = dot(expert_in[...], wu[:, columns])
        silu = gate_value / (1.0 + jnp.exp(-gate_value))
        hidden[:, columns] = (silu * up_value * my_gate).astype(jnp.bfloat16)
        return carry

    lax.fori_loop(0, ff_share // COLUMNS, hidden_step, 0)

    for c in weights[2 * WEIGHT_PARTS :]:
        c.wait()

    step = width // DOWN_PARTS

    pairs = []

    def spread_sums(part):
        arrived(pair_sem.at[part], p5.at[part])
        both = s5[part, core].astype(jnp.float32) + p5[part].astype(jnp.float32)
        t5[part] = both.astype(jnp.bfloat16)
        for d in range(n - 2, 0, -2):
            send(4 + part, d, t5.at[part, peer_at[d] // 2], r5.at[part, chip])
        r5[part, chip] = t5[part, chip]

    for part in range(DOWN_PARTS):
        partial = dot(hidden[...], wd[:, part * step : (part + 1) * step])
        for peer in range(n):
            s5[part, peer % 2, peer // 2] = partial[peer * rows : (peer + 1) * rows].astype(
                jnp.bfloat16
            )
        pairs.append(
            pltpu.make_async_remote_copy(
                src_ref=s5.at[part, 1 - core],
                dst_ref=p5.at[part],
                send_sem=pair_send_sem.at[part],
                recv_sem=pair_sem.at[part],
                device_id={"ep": peer_at[1]},
                device_id_type=pl.DeviceIdType.MESH,
            )
        )
        pairs[-1].start()
        if part:
            spread_sums(part - 1)
    spread_sums(DOWN_PARTS - 1)
    for part in range(DOWN_PARTS):
        arrived(recv_sem.at[4 + part], r5.at[part, other_chips])
        total = own_mixed[:, part * step : (part + 1) * step]
        for peer in range(n // 2):
            total = total + r5[part, peer].astype(jnp.float32)
        out_ref[:, part * step : (part + 1) * step] = total.astype(jnp.bfloat16)
    results[0].start()
    for stage, blocks in enumerate((s1, None, r3, r4)):
        if blocks is not None:
            arrived(send_sem.at[stage], blocks.at[others])
    arrived(send_sem.at[1], t2.at[other_chips])
    pair.wait_send()
    for part in range(DOWN_PARTS):
        pairs[part].wait_send()
        arrived(send_sem.at[4 + part], t5.at[part, other_chips])
    for c in results:
        c.wait()


def local(
    n,
    tokens,
    lengths,
    cache_key,
    cache_value,
    routes,
    route_logits,
    mix_gain,
    query_gain,
    key_gain,
    head_bias,
    w_query,
    w_key,
    w_value,
    w_out,
    ffn_gain,
    w_gate,
    w_up,
    w_down,
):
    rows, width = tokens.shape
    all_rows = rows * n
    share = width // n
    q_width, k_width = w_query.shape[1], w_key.shape[1]
    wide = q_width + k_width + w_value.shape[1]
    stages = 4 + DOWN_PARTS
    anywhere = pl.BlockSpec(memory_space=pl.ANY)
    smem = pl.BlockSpec(memory_space=pltpu.SMEM)
    bf16, f32 = jnp.bfloat16, jnp.float32

    def like(array):
        return pltpu.VMEM(array.shape, array.dtype)

    flops = 2 * all_rows * 3 * w_gate.shape[0] * w_gate.shape[1]
    shapes = ((rows, width), (rows, k_width), (rows, w_value.shape[1]))
    return pl.pallas_call(
        functools.partial(fused, n),
        out_shape=tuple(pltpu.VMEM(shape, bf16) for shape in shapes),
        in_specs=[anywhere, smem] + [anywhere] * 16,
        out_specs=(anywhere,) * 3,
        scratch_shapes=[
            like(tokens),
            pltpu.VMEM(routes.shape[::-1], routes.dtype),
            pltpu.VMEM(route_logits.shape[::-1], f32),
            pltpu.VMEM((1, width), f32),
            pltpu.VMEM((1, HEAD_DIM), f32),
            pltpu.VMEM((1, HEAD_DIM), f32),
            pltpu.VMEM((1, HEADS), f32),
            pltpu.VMEM((1, width), f32),
            *(pltpu.VMEM(shape, bf16) for shape in shapes),
            like(w_query),
            like(w_key),
            like(w_value),
            like(w_out),
            like(cache_key),
            like(cache_value),
            like(w_gate),
            like(w_up),
            like(w_down),
            pltpu.VMEM((n, 2 * rows, share), bf16),
            pltpu.VMEM((n, 2 * rows, share), bf16),
            pltpu.VMEM((2, n // 2, rows, wide), bf16),
            pltpu.VMEM((n // 2, rows, wide), bf16),
            pltpu.VMEM((n // 2, rows, wide), bf16),
            pltpu.VMEM((n // 2, rows, wide), bf16),
            pltpu.VMEM((n, rows, q_width), bf16),
            pltpu.VMEM((n, all_rows, share), bf16),
            pltpu.VMEM((DOWN_PARTS, 2, n // 2, rows, width // DOWN_PARTS), bf16),
            pltpu.VMEM((DOWN_PARTS, n // 2, rows, width // DOWN_PARTS), bf16),
            pltpu.VMEM((DOWN_PARTS, n // 2, rows, width // DOWN_PARTS), bf16),
            pltpu.VMEM((DOWN_PARTS, n // 2, rows, width // DOWN_PARTS), bf16),
            pltpu.VMEM((all_rows, share), f32),
            pltpu.VMEM((all_rows, share), f32),
            pltpu.VMEM((all_rows, q_width), f32),
            pltpu.VMEM((all_rows, width), bf16),
            pltpu.VMEM((all_rows, w_gate.shape[1]), bf16),
            pltpu.SemaphoreType.DMA((8,)),
            pltpu.SemaphoreType.DMA((3,)),
            pltpu.SemaphoreType.DMA((4,)),
            pltpu.SemaphoreType.DMA((rows,)),
            pltpu.SemaphoreType.DMA((rows,)),
            pltpu.SemaphoreType.DMA((3, WEIGHT_PARTS)),
            pltpu.SemaphoreType.DMA((stages,)),
            pltpu.SemaphoreType.DMA((stages,)),
            pltpu.SemaphoreType.DMA((n,)),
            pltpu.SemaphoreType.DMA((DOWN_PARTS + 1,)),
            pltpu.SemaphoreType.DMA((DOWN_PARTS + 1,)),
        ],
        compiler_params=pltpu.CompilerParams(
            collective_id=0, has_side_effects=True, vmem_limit_bytes=60 * 1024 * 1024
        ),
        cost_estimate=pl.CostEstimate(flops=flops, bytes_accessed=flops // all_rows, transcendentals=0),
    )(
        tokens,
        lengths,
        cache_key,
        cache_value,
        routes.T,
        route_logits.T,
        mix_gain.reshape(1, -1),
        query_gain.reshape(1, -1),
        key_gain.reshape(1, -1),
        head_bias.reshape(1, -1),
        w_query,
        w_key,
        w_value,
        w_out,
        ffn_gain.reshape(1, -1),
        w_gate,
        w_up,
        w_down,
    )


def solution(mesh):
    n = mesh.shape["ep"]

    def body(*arrays):
        tokens, w_gate = arrays[0], arrays[15]
        share = tokens.shape[1] // n
        if share == 128 and n & (n - 1) == 0 and w_gate.shape[1] % COLUMNS == 0:
            return local(n, *arrays)
        return plain(*arrays)

    return jax.shard_map(
        body,
        mesh=mesh,
        in_specs=(
            P(("grp", "ep"), None),
            P(("grp", "ep")),
            P(("grp", "ep"), None, None),
            P(("grp", "ep"), None, None),
            P(("grp", "ep"), None),
            P(("grp", "ep"), None),
            P(),
            P(),
            P(),
            P(),
            P("ep", None),
            P("ep", None),
            P("ep", None),
            P(None, "ep"),
            P(),
            P(None, "ep"),
            P(None, "ep"),
            P("ep", None),
        ),
        out_specs=(P(("grp", "ep"), None), P(("grp", "ep"), None), P(("grp", "ep"), None)),
        check_vma=False,
    )
```

```python
import functools

import jax
import jax.numpy as jnp
from jax import lax
from jax.experimental import pallas as pl
from jax.experimental.pallas import tpu as pltpu
from jax.sharding import PartitionSpec as P

HEADS = 16
KV_HEADS = 4
HEAD_DIM = 64
FF = 7168
EXPERTS = 4


EPSILON = 1e-06


def rms_scaled(values, gain):
    return values * lax.rsqrt(jnp.mean(values * values, axis=-1, keepdims=True) + EPSILON) * gain


def route_weights(routes, route_logits):
    experts_iota = jnp.arange(EXPERTS, dtype=jnp.int32)[None, :]
    first_share = jax.nn.sigmoid(route_logits[:, 0:1] - route_logits[:, 1:2])
    second_share = jax.nn.sigmoid(route_logits[:, 1:2] - route_logits[:, 0:1])
    return jnp.where(routes[:, 0:1] == experts_iota, first_share, 0.0) + jnp.where(
        routes[:, 1:2] == experts_iota, second_share, 0.0
    )


def stick_attend(queries, lengths, cache_key, cache_value, query_gain, head_bias):
    batch_rows = queries.shape[0]
    cache_len = cache_key.shape[1]
    group_size = HEADS // KV_HEADS
    normed_query = rms_scaled(queries.reshape(batch_rows, HEADS, HEAD_DIM), query_gain).astype(
        jnp.bfloat16
    )
    normed_query = normed_query.reshape(batch_rows, KV_HEADS, group_size, HEAD_DIM)
    key_heads = cache_key.reshape(batch_rows, cache_len, KV_HEADS, HEAD_DIM)
    value_heads = cache_value.reshape(batch_rows, cache_len, KV_HEADS, HEAD_DIM)
    scores = jnp.einsum(
        "bkgd,blkd->bkgl", normed_query, key_heads, preferred_element_type=jnp.float32
    ) * HEAD_DIM ** (-0.5)
    scores = scores + head_bias.reshape(KV_HEADS, group_size)[None, :, :, None]
    live_mask = (
        jnp.arange(cache_len, dtype=jnp.int32)[None, None, None, :] < lengths[:, None, None, None]
    )
    remain = jnp.where(live_mask, jax.nn.log_sigmoid(-scores), 0.0)
    after_sum = lax.cumsum(remain, axis=3, reverse=True) - remain
    weights = jnp.where(live_mask, jnp.exp(jax.nn.log_sigmoid(scores) + after_sum), 0.0).astype(
        jnp.bfloat16
    )
    attended = jnp.einsum(
        "bkgl,blkd->bkgd", weights, value_heads, preferred_element_type=jnp.float32
    )
    return attended.reshape(batch_rows, HEADS * HEAD_DIM).astype(jnp.bfloat16)


def plain(
    tokens,
    lengths,
    cache_key,
    cache_value,
    routes,
    route_logits,
    mix_gain,
    query_gain,
    key_gain,
    head_bias,
    w_query,
    w_key,
    w_value,
    w_out,
    ffn_gain,
    w_gate,
    w_up,
    w_down,
):
    token_rows = tokens.shape[0]
    key_width = w_key.shape[1]
    as_float = tokens.astype(jnp.float32)
    normed = rms_scaled(as_float, mix_gain).astype(jnp.bfloat16)
    pieces = (
        lax.all_gather(w_query, "ep", axis=0, tiled=True),
        lax.all_gather(w_key, "ep", axis=0, tiled=True),
        lax.all_gather(w_value, "ep", axis=0, tiled=True),
    )
    queries, fresh_key, fresh_value = tuple(
        (jnp.dot(normed, weight, preferred_element_type=jnp.float32) for weight in pieces)
    )
    new_key = rms_scaled(fresh_key.reshape(token_rows, KV_HEADS, HEAD_DIM), key_gain)
    new_key = new_key.reshape(token_rows, key_width).astype(jnp.bfloat16)
    new_value = fresh_value.astype(jnp.bfloat16)
    attended = stick_attend(queries, lengths, cache_key, cache_value, query_gain, head_bias)
    mixed = as_float + jnp.dot(
        attended,
        lax.all_gather(w_out, "ep", axis=1, tiled=True),
        preferred_element_type=jnp.float32,
    )
    expert_in = rms_scaled(mixed, ffn_gain).astype(jnp.bfloat16)
    every_gate = lax.all_gather(route_weights(routes, route_logits), "ep", axis=0, tiled=True)
    ff_share = w_gate.shape[1]
    my_expert = lax.axis_index("ep") // (FF // ff_share)
    my_gate = lax.dynamic_slice_in_dim(every_gate, my_expert, 1, 1)
    input_rows = lax.all_gather(expert_in, "ep", axis=0, tiled=True)
    gate_value = jnp.dot(input_rows, w_gate, preferred_element_type=jnp.float32)
    up_value = jnp.dot(input_rows, w_up, preferred_element_type=jnp.float32)
    hidden = (jax.nn.silu(gate_value) * up_value * my_gate).astype(jnp.bfloat16)
    expert_sum = lax.psum_scatter(
        jnp.dot(hidden, w_down, preferred_element_type=jnp.float32),
        "ep",
        scatter_dimension=0,
        tiled=True,
    )
    return ((mixed + expert_sum).astype(jnp.bfloat16), new_key, new_value)


WEIGHT_PARTS = 2
DOWN_PARTS = 4
COLUMNS = 256


def dot(left, right):
    return jnp.dot(left, right, preferred_element_type=jnp.float32)


def iota(shape, dim):
    return lax.broadcasted_iota(jnp.int32, shape, dim)


def column(row):
    square = (row.shape[1], row.shape[1])
    return jnp.sum(
        jnp.where(iota(square, 0) == iota(square, 1), jnp.broadcast_to(row, square), 0.0),
        axis=1,
        keepdims=True,
    )


def finish(*refs):
    half = len(refs) // 2
    copies = [
        pltpu.make_async_copy(refs[i], refs[half + i], refs[-1].at[i]) for i in range(half)
    ]
    for copy in copies:
        copy.start()
    for copy in copies:
        copy.wait()


def fused(
    n,
    tokens_hbm,
    lengths_ref,
    ck_hbm,
    cv_hbm,
    routes_hbm,
    logits_hbm,
    mix_gain_hbm,
    query_gain_hbm,
    key_gain_hbm,
    head_bias_hbm,
    wq_hbm,
    wk_hbm,
    wv_hbm,
    wo_hbm,
    ffn_gain_hbm,
    wg_hbm,
    wu_hbm,
    wd_hbm,
    out_any,
    new_key_any,
    new_value_any,
    tokens_ref,
    routes_ref,
    logits_ref,
    mix_gain_ref,
    query_gain_ref,
    key_gain_ref,
    head_bias_ref,
    ffn_gain_ref,
    out_ref,
    new_key_ref,
    new_value_ref,
    wq,
    wk,
    wv,
    wo,
    ck,
    cv,
    wg,
    wu,
    wd,
    s1,
    r1,
    s2,
    p2,
    t2,
    r2,
    r3,
    r4,
    s5,
    p5,
    t5,
    r5,
    token_cols,
    aux_rows,
    attended_rows,
    expert_in,
    hidden,
    operand_sem,
    result_sem,
    small_sem,
    key_sem,
    value_sem,
    weight_sem,
    send_sem,
    recv_sem,
    block_sem,
    pair_send_sem,
    pair_sem,
):
    me = lax.axis_index("ep")
    rows, width = tokens_ref.shape
    all_rows = rows * n
    share = width // n
    q_width = wq.shape[1]
    k_width = wk.shape[1]
    cache_len = ck.shape[1]
    group_size = HEADS // KV_HEADS
    ff_share = wg.shape[1]
    my_expert = me // (FF // ff_share)

    barrier = pltpu.get_barrier_semaphore()
    peer_at = [me]
    for d in range(1, n):
        bit = d.bit_length() - 1
        flip = 2**bit * (1 - 2 * ((me // 2**bit) % 2))
        peer_at.append(peer_at[d - 2**bit] + flip)
    furthest_first = range(n - 1, 0, -1)
    core, chip = me % 2, me // 2
    for d in furthest_first:
        pl.semaphore_signal(
            barrier,
            inc=1,
            device_id={"ep": peer_at[d]},
            device_id_type=pl.DeviceIdType.MESH,
        )

    operands = [
        pltpu.make_async_copy(a, b, operand_sem.at[i])
        for i, (a, b) in enumerate(
            (
                (tokens_hbm, tokens_ref),
                (routes_hbm, routes_ref),
                (logits_hbm, logits_ref),
                (mix_gain_hbm, mix_gain_ref),
                (query_gain_hbm, query_gain_ref),
                (key_gain_hbm, key_gain_ref),
                (head_bias_hbm, head_bias_ref),
                (ffn_gain_hbm, ffn_gain_ref),
            )
        )
    ]
    for c in operands:
        c.start()

    small = [
        pltpu.make_async_copy(a, b, small_sem.at[i])
        for i, (a, b) in enumerate(((wq_hbm, wq), (wk_hbm, wk), (wv_hbm, wv), (wo_hbm, wo)))
    ]
    for c in small[:3]:
        c.start()
    keys = [pltpu.make_async_copy(ck_hbm.at[b], ck.at[b], key_sem.at[b]) for b in range(rows)]
    values = [pltpu.make_async_copy(cv_hbm.at[b], cv.at[b], value_sem.at[b]) for b in range(rows)]
    weights = []
    for which, (a, b) in enumerate(((wg_hbm, wg), (wu_hbm, wu), (wd_hbm, wd))):
        step = b.shape[0] // WEIGHT_PARTS
        for part in range(WEIGHT_PARTS):
            piece = pl.ds(part * step, step)
            weights.append(
                pltpu.make_async_copy(
                    a.at[piece], b.at[piece], weight_sem.at[which, part]
                )
            )

    results = [
        pltpu.make_async_copy(a, b, result_sem.at[i])
        for i, (a, b) in enumerate(
            ((out_ref, out_any), (new_key_ref, new_key_any), (new_value_ref, new_value_any))
        )
    ]
    for c in operands:
        c.wait()


    def send(stage, d, source, target, arrival=None):
        copy = pltpu.make_async_remote_copy(
            src_ref=source,
            dst_ref=target,
            send_sem=send_sem.at[stage],
            recv_sem=recv_sem.at[stage] if arrival is None else arrival,
            device_id={"ep": peer_at[d]},
            device_id_type=pl.DeviceIdType.MESH,
        )
        copy.start()

    def arrived(sem, blocks):
        pltpu.make_async_copy(blocks, blocks, sem).wait()

    others = pl.ds(0, n - 1)
    other_chips = pl.ds(0, n // 2 - 1)

    as_float = tokens_ref[...].astype(jnp.float32)
    scale = lax.rsqrt(jnp.mean(as_float * as_float, axis=1, keepdims=True) + EPSILON)
    lane = iota((rows, 128), 1)
    logit_gap = column(logits_ref[0:1] - logits_ref[1:2])
    chosen = [column(routes_ref[i : i + 1].astype(jnp.float32)) for i in range(2)]
    first_share = 1.0 / (1.0 + jnp.exp(-logit_gap))
    second_share = 1.0 / (1.0 + jnp.exp(logit_gap))
    expert_lane = (lane % EXPERTS).astype(jnp.float32)
    gates = jnp.where(chosen[0] == expert_lane, first_share, 0.0) + jnp.where(
        chosen[1] == expert_lane, second_share, 0.0
    )
    aux = jnp.where(lane < 3 * EXPERTS, gates, scale)
    high = aux.astype(jnp.bfloat16).astype(jnp.float32)
    middle = (aux - high).astype(jnp.bfloat16).astype(jnp.float32)
    low = aux - high - middle
    term = jnp.where(lane < 3 * EXPERTS, lane // EXPERTS, lane - 3 * EXPERTS)
    aux = jnp.where(term == 0, high, jnp.where(term == 1, middle, low))
    for peer in range(n):
        block = jnp.concatenate(
            [as_float[:, peer * share : (peer + 1) * share], aux], axis=0
        ).astype(jnp.bfloat16)
        s1[peer] = block
    pl.semaphore_wait(barrier, n - 1)
    for d in furthest_first:
        send(0, d, s1.at[peer_at[d]], r1.at[me])
    for c in keys + values + small[3:]:
        c.start()
    r1[me] = s1[me]
    for c in small[:3]:
        c.wait()
    arrived(recv_sem.at[0], r1.at[others])
    for c in weights:
        c.start()
    for peer in range(n):
        block = r1[peer].astype(jnp.float32)
        token_cols[peer * rows : (peer + 1) * rows, :] = block[:rows]
        aux_rows[peer * rows : (peer + 1) * rows, :] = block[rows:]
    aux = aux_rows[...]
    lane = iota(aux.shape, 1)
    row_scale = jnp.sum(
        jnp.where((lane >= 3 * EXPERTS) & (lane < 3 * EXPERTS + 3), aux, 0.0), axis=1, keepdims=True
    )
    my_gate = jnp.sum(
        jnp.where((lane < 3 * EXPERTS) & (lane % EXPERTS == my_expert), aux, 0.0),
        axis=1,
        keepdims=True,
    )
    my_gain = mix_gain_ref[:, pl.ds(pl.multiple_of(me * share, share), share)]
    normed = (token_cols[...] * row_scale * my_gain).astype(jnp.bfloat16)

    for weight, start in ((wq, 0), (wk, q_width), (wv, q_width + k_width)):
        partial = dot(normed, weight[...])
        for peer in range(n):
            s2[peer % 2, peer // 2, :, start : start + weight.shape[1]] = partial[
                peer * rows : (peer + 1) * rows
            ].astype(jnp.bfloat16)
    pair = pltpu.make_async_remote_copy(
        src_ref=s2.at[1 - core],
        dst_ref=p2,
        send_sem=pair_send_sem.at[DOWN_PARTS],
        recv_sem=pair_sem.at[DOWN_PARTS],
        device_id={"ep": peer_at[1]},
        device_id_type=pl.DeviceIdType.MESH,
    )
    pair.start()

    head_of_lane = iota((HEADS, q_width), 1) // HEAD_DIM
    own_lane = head_of_lane == iota((HEADS, q_width), 0)
    source_lane = iota((q_width, k_width), 0)
    target_lane = iota((q_width, k_width), 1)
    fold = jnp.where(
        (source_lane // (HEAD_DIM * group_size) == target_lane // HEAD_DIM)
        & (source_lane % HEAD_DIM == target_lane % HEAD_DIM),
        1.0,
        0.0,
    ).astype(jnp.bfloat16)
    later = jnp.where(
        iota((COLUMNS, COLUMNS), 0) > iota((COLUMNS, COLUMNS), 1), 1.0, 0.0
    ).astype(jnp.bfloat16)
    query_gain = jnp.concatenate([query_gain_ref[...]] * HEADS, axis=1)
    key_gain = jnp.concatenate([key_gain_ref[...]] * KV_HEADS, axis=1)

    pair.wait_recv()
    t2[...] = (s2[core].astype(jnp.float32) + p2[...].astype(jnp.float32)).astype(jnp.bfloat16)
    for d in range(n - 2, 0, -2):
        send(1, d, t2.at[peer_at[d] // 2], r2.at[chip])
    r2[chip] = t2[chip]
    arrived(recv_sem.at[1], r2.at[other_chips])
    total = r2[0].astype(jnp.float32)
    for peer in range(1, n // 2):
        total = total + r2[peer].astype(jnp.float32)
    queries = total[:, :q_width]
    fresh_key = total[:, q_width : q_width + k_width]
    new_value_ref[...] = total[:, q_width + k_width :].astype(jnp.bfloat16)
    squares = fresh_key * fresh_key
    key_lane = iota(squares.shape, 1) // HEAD_DIM
    key_scale = jnp.zeros_like(squares)
    for g in range(KV_HEADS):
        mean = jnp.sum(jnp.where(key_lane == g, squares, 0.0), axis=1, keepdims=True) / HEAD_DIM
        key_scale = jnp.where(key_lane == g, lax.rsqrt(mean + EPSILON), key_scale)
    new_key_ref[...] = (fresh_key * key_scale * key_gain).astype(jnp.bfloat16)

    for c in results[1:]:
        c.start()

    spread = []
    for b in range(rows):
        wide = jnp.where(own_lane, jnp.broadcast_to(queries[b : b + 1], own_lane.shape), 0.0)
        mean = jnp.sum(wide * wide, axis=1, keepdims=True) / HEAD_DIM
        spread.append((wide * lax.rsqrt(mean + EPSILON) * query_gain).astype(jnp.bfloat16))
    folded = dot(jnp.concatenate(spread, axis=0), fold).astype(jnp.bfloat16)
    blocks = cache_len // COLUMNS
    head_rows = rows * HEADS
    head_bias = jnp.concatenate([column(head_bias_ref[...])] * rows, axis=0)
    row_of = iota((head_rows, 1), 0) // HEADS
    lengths = jnp.zeros((head_rows, 1), jnp.int32)
    for b in range(rows):
        lengths = jnp.where(row_of == b, lengths_ref[b], lengths)
    live = iota((head_rows, cache_len), 1) < lengths
    for c in keys + values:
        c.wait()
    scores = jnp.concatenate(
        [
            lax.dot_general(
                folded[b * HEADS : (b + 1) * HEADS],
                ck[b],
                (((1,), (1,)), ((), ())),
                preferred_element_type=jnp.float32,
            )
            for b in range(rows)
        ],
        axis=0,
    )
    scores = scores * HEAD_DIM ** (-0.5) + head_bias
    tail_log = jnp.log1p(jnp.exp(-jnp.abs(scores)))
    remain = jnp.where(live, jnp.minimum(-scores, 0.0) - tail_log, 0.0)
    after = [None] * blocks
    carry = jnp.zeros((head_rows, 1), jnp.float32)
    for i in reversed(range(blocks)):
        block = remain[:, i * COLUMNS : (i + 1) * COLUMNS]
        high = block.astype(jnp.bfloat16)
        low = (block - high.astype(jnp.float32)).astype(jnp.bfloat16)
        after[i] = dot(high, later) + dot(low, later) + carry
        carry = carry + jnp.sum(block, axis=1, keepdims=True)
    after_sum = jnp.concatenate(after, axis=1)
    chance = jnp.exp(jnp.minimum(scores, 0.0) - tail_log + after_sum)
    weight = jnp.where(live, chance, 0.0).astype(jnp.bfloat16)
    mixed_heads = jnp.concatenate(
        [dot(weight[b * HEADS : (b + 1) * HEADS], cv[b]) for b in range(rows)], axis=0
    )
    own_group = (
        iota((head_rows, k_width), 1) // HEAD_DIM
        == iota((head_rows, k_width), 0) % HEADS // group_size
    )
    heads = jnp.where(own_group, mixed_heads, 0.0).astype(jnp.bfloat16)
    unfolded = lax.dot_general(
        heads,
        fold,
        (((1,), (1,)), ((), ())),
        preferred_element_type=jnp.float32,
    )
    attended = [
        jnp.sum(
            jnp.where(own_lane, unfolded[b * HEADS : (b + 1) * HEADS], 0.0), axis=0, keepdims=True
        )
        for b in range(rows)
    ]
    r3[me] = jnp.concatenate(attended, axis=0).astype(jnp.bfloat16)

    for d in furthest_first:
        send(2, d, r3.at[me], r3.at[me])
    small[3].wait()
    arrived(recv_sem.at[2], r3.at[others])
    for peer in range(n):
        attended_rows[peer * rows : (peer + 1) * rows, :] = r3[peer].astype(jnp.float32)
    mixed = token_cols[...] + dot(attended_rows[...].astype(jnp.bfloat16), wo[...])
    r4[me] = mixed.astype(jnp.bfloat16)

    for d in range(n - 2, 0, -2):
        send(3, d, r4.at[me], r4.at[me], block_sem.at[me])
    send(3, 1, r4.at[me], r4.at[me], block_sem.at[me])
    for d in range(2, n, 2):
        source = peer_at[d]
        arrived(block_sem.at[source], r4.at[source])
        send(3, 1, r4.at[source], r4.at[source], block_sem.at[source])
    for d in range(1, n, 2):
        source = peer_at[d]
        arrived(block_sem.at[source], r4.at[source])
    squares = jnp.zeros((all_rows, share), jnp.float32)
    for peer in range(n):
        block = r4[peer].astype(jnp.float32)
        squares = squares + block * block
    scale = lax.rsqrt(jnp.sum(squares, axis=1, keepdims=True) / width + EPSILON)
    pick = jnp.where(
        iota((8, all_rows), 1) == iota((8, all_rows), 0) + me * rows, 1.0, 0.0
    ).astype(jnp.bfloat16)
    own_mixed = []
    for peer in range(n):
        columns = slice(peer * share, (peer + 1) * share)
        block = r4[peer]
        own_mixed.append(dot(pick, block)[:rows])
        expert_in[:, columns] = (
            block.astype(jnp.float32) * scale * ffn_gain_ref[:, columns]
        ).astype(jnp.bfloat16)
    own_mixed = jnp.concatenate(own_mixed, axis=1)

    for c in weights[: 2 * WEIGHT_PARTS]:
        c.wait()

    def hidden_step(i, carry):
        columns = pl.ds(pl.multiple_of(i * COLUMNS, COLUMNS), COLUMNS)
        gate_value = dot(expert_in[...], wg[:, columns])
        up_value = dot(expert_in[...], wu[:, columns])
        silu = gate_value / (1.0 + jnp.exp(-gate_value))
        hidden[:, columns] = (silu * up_value * my_gate).astype(jnp.bfloat16)
        return carry

    lax.fori_loop(0, ff_share // COLUMNS, hidden_step, 0)

    for c in weights[2 * WEIGHT_PARTS :]:
        c.wait()

    step = width // DOWN_PARTS

    pairs = []

    def spread_sums(part):
        arrived(pair_sem.at[part], p5.at[part])
        both = s5[part, core].astype(jnp.float32) + p5[part].astype(jnp.float32)
        t5[part] = both.astype(jnp.bfloat16)
        for d in range(n - 2, 0, -2):
            send(4 + part, d, t5.at[part, peer_at[d] // 2], r5.at[part, chip])
        r5[part, chip] = t5[part, chip]

    for part in range(DOWN_PARTS):
        partial = dot(hidden[...], wd[:, part * step : (part + 1) * step])
        for peer in range(n):
            s5[part, peer % 2, peer // 2] = partial[peer * rows : (peer + 1) * rows].astype(
                jnp.bfloat16
            )
        pairs.append(
            pltpu.make_async_remote_copy(
                src_ref=s5.at[part, 1 - core],
                dst_ref=p5.at[part],
                send_sem=pair_send_sem.at[part],
                recv_sem=pair_sem.at[part],
                device_id={"ep": peer_at[1]},
                device_id_type=pl.DeviceIdType.MESH,
            )
        )
        pairs[-1].start()
        if part:
            spread_sums(part - 1)
    spread_sums(DOWN_PARTS - 1)
    for part in range(DOWN_PARTS):
        arrived(recv_sem.at[4 + part], r5.at[part, other_chips])
        total = own_mixed[:, part * step : (part + 1) * step]
        for peer in range(n // 2):
            total = total + r5[part, peer].astype(jnp.float32)
        out_ref[:, part * step : (part + 1) * step] = total.astype(jnp.bfloat16)
    results[0].start()
    for stage, blocks in enumerate((s1, None, r3, r4)):
        if blocks is not None:
            arrived(send_sem.at[stage], blocks.at[others])
    arrived(send_sem.at[1], t2.at[other_chips])
    pair.wait_send()
    for part in range(DOWN_PARTS):
        pairs[part].wait_send()
        arrived(send_sem.at[4 + part], t5.at[part, other_chips])
    for c in results:
        c.wait()


def local(
    n,
    tokens,
    lengths,
    cache_key,
    cache_value,
    routes,
    route_logits,
    mix_gain,
    query_gain,
    key_gain,
    head_bias,
    w_query,
    w_key,
    w_value,
    w_out,
    ffn_gain,
    w_gate,
    w_up,
    w_down,
):
    rows, width = tokens.shape
    all_rows = rows * n
    share = width // n
    q_width, k_width = w_query.shape[1], w_key.shape[1]
    wide = q_width + k_width + w_value.shape[1]
    stages = 4 + DOWN_PARTS
    anywhere = pl.BlockSpec(memory_space=pl.ANY)
    smem = pl.BlockSpec(memory_space=pltpu.SMEM)
    bf16, f32 = jnp.bfloat16, jnp.float32

    def like(array):
        return pltpu.VMEM(array.shape, array.dtype)

    flops = 2 * all_rows * 3 * w_gate.shape[0] * w_gate.shape[1]
    shapes = ((rows, width), (rows, k_width), (rows, w_value.shape[1]))
    results = pl.pallas_call(
        functools.partial(fused, n),
        out_shape=tuple(pltpu.VMEM(shape, bf16) for shape in shapes),
        in_specs=[anywhere, smem] + [anywhere] * 16,
        out_specs=(anywhere,) * 3,
        scratch_shapes=[
            like(tokens),
            pltpu.VMEM(routes.shape[::-1], routes.dtype),
            pltpu.VMEM(route_logits.shape[::-1], f32),
            pltpu.VMEM((1, width), f32),
            pltpu.VMEM((1, HEAD_DIM), f32),
            pltpu.VMEM((1, HEAD_DIM), f32),
            pltpu.VMEM((1, HEADS), f32),
            pltpu.VMEM((1, width), f32),
            *(pltpu.VMEM(shape, bf16) for shape in shapes),
            like(w_query),
            like(w_key),
            like(w_value),
            like(w_out),
            like(cache_key),
            like(cache_value),
            like(w_gate),
            like(w_up),
            like(w_down),
            pltpu.VMEM((n, 2 * rows, share), bf16),
            pltpu.VMEM((n, 2 * rows, share), bf16),
            pltpu.VMEM((2, n // 2, rows, wide), bf16),
            pltpu.VMEM((n // 2, rows, wide), bf16),
            pltpu.VMEM((n // 2, rows, wide), bf16),
            pltpu.VMEM((n // 2, rows, wide), bf16),
            pltpu.VMEM((n, rows, q_width), bf16),
            pltpu.VMEM((n, all_rows, share), bf16),
            pltpu.VMEM((DOWN_PARTS, 2, n // 2, rows, width // DOWN_PARTS), bf16),
            pltpu.VMEM((DOWN_PARTS, n // 2, rows, width // DOWN_PARTS), bf16),
            pltpu.VMEM((DOWN_PARTS, n // 2, rows, width // DOWN_PARTS), bf16),
            pltpu.VMEM((DOWN_PARTS, n // 2, rows, width // DOWN_PARTS), bf16),
            pltpu.VMEM((all_rows, share), f32),
            pltpu.VMEM((all_rows, share), f32),
            pltpu.VMEM((all_rows, q_width), f32),
            pltpu.VMEM((all_rows, width), bf16),
            pltpu.VMEM((all_rows, w_gate.shape[1]), bf16),
            pltpu.SemaphoreType.DMA((8,)),
            pltpu.SemaphoreType.DMA((3,)),
            pltpu.SemaphoreType.DMA((4,)),
            pltpu.SemaphoreType.DMA((rows,)),
            pltpu.SemaphoreType.DMA((rows,)),
            pltpu.SemaphoreType.DMA((3, WEIGHT_PARTS)),
            pltpu.SemaphoreType.DMA((stages,)),
            pltpu.SemaphoreType.DMA((stages,)),
            pltpu.SemaphoreType.DMA((n,)),
            pltpu.SemaphoreType.DMA((DOWN_PARTS + 1,)),
            pltpu.SemaphoreType.DMA((DOWN_PARTS + 1,)),
        ],
        compiler_params=pltpu.CompilerParams(
            collective_id=0, has_side_effects=True, vmem_limit_bytes=60 * 1024 * 1024
        ),
        cost_estimate=pl.CostEstimate(flops=flops, bytes_accessed=flops // all_rows, transcendentals=0),
    )(
        tokens,
        lengths,
        cache_key,
        cache_value,
        routes.T,
        route_logits.T,
        mix_gain.reshape(1, -1),
        query_gain.reshape(1, -1),
        key_gain.reshape(1, -1),
        head_bias.reshape(1, -1),
        w_query,
        w_key,
        w_value,
        w_out,
        ffn_gain.reshape(1, -1),
        w_gate,
        w_up,
        w_down,
    )
    return pl.pallas_call(
        finish,
        out_shape=tuple(jax.ShapeDtypeStruct(shape, bf16) for shape in shapes),
        in_specs=[anywhere] * len(shapes),
        out_specs=(anywhere,) * len(shapes),
        scratch_shapes=[pltpu.SemaphoreType.DMA((len(shapes),))],
    )(*(pltpu.with_memory_space_constraint(result, pltpu.VMEM) for result in results))


def solution(mesh):
    n = mesh.shape["ep"]

    def body(*arrays):
        tokens, w_gate = arrays[0], arrays[15]
        share = tokens.shape[1] // n
        if share == 128 and n & (n - 1) == 0 and w_gate.shape[1] % COLUMNS == 0:
            return local(n, *arrays)
        return plain(*arrays)

    return jax.shard_map(
        body,
        mesh=mesh,
        in_specs=(
            P(("grp", "ep"), None),
            P(("grp", "ep")),
            P(("grp", "ep"), None, None),
            P(("grp", "ep"), None, None),
            P(("grp", "ep"), None),
            P(("grp", "ep"), None),
            P(),
            P(),
            P(),
            P(),
            P("ep", None),
            P("ep", None),
            P("ep", None),
            P(None, "ep"),
            P(),
            P(None, "ep"),
            P(None, "ep"),
            P("ep", None),
        ),
        out_specs=(P(("grp", "ep"), None), P(("grp", "ep"), None), P(("grp", "ep"), None)),
        check_vma=False,
    )
```
